32 devices in a mesh: ep: 8 (over z, x), tp: 4 (over y, core).
Axes of the slice: x: 2, y: 2, z: 4, core: 2. Of those that a mesh axis runs over, the one named last changes fastest.
Arguments:
- query_rows: bfloat16 [2048, 1024], P('ep', 'tp'), may hold values from -8 to 8
- key_rows: bfloat16 [2048, 256], P('ep', 'tp'), may hold values from -8 to 8
- value_rows: bfloat16 [2048, 256], P('ep', 'tp'), may hold values from -16 to 16
- query_gain: float32 [64], replicated, may hold values from 0.5 to 7.5
- key_gain: float32 [64], replicated, may hold values from 0.5 to 7.5
- moe_tokens: bfloat16 [4096, 2048], P(('ep', 'tp')), may hold values from -6 to 6
- norm_gain: float32 [2048], replicated, may hold values from 0.1 to 1.9
- routes: int32 [4096, 2], P('ep'), may hold values from 0 to 7, all different within a row; in each aligned block of 128 rows (0 to 127, 128 to 255, ...) at most 64 rows name the same one
- route_weights: float32 [4096, 2], P('ep'), may hold values from 0.1 to 1
- expert_gate: bfloat16 [8, 2048, 1024], P('ep', None, 'tp'), may hold values from -0.125 to 0.125
- expert_up: bfloat16 [8, 2048, 1024], P('ep', None, 'tp'), may hold values from -0.125 to 0.125
- expert_down: bfloat16 [8, 1024, 2048], P('ep', 'tp'), may hold values from -0.1875 to 0.1875
- shared_gate: bfloat16 [2048, 1024], P(None, 'tp'), may hold values from -0.125 to 0.125
- shared_up: bfloat16 [2048, 1024], P(None, 'tp'), may hold values from -0.125 to 0.125
- shared_down: bfloat16 [1024, 2048], P('tp'), may hold values from -0.1875 to 0.1875
Outputs:
- attn_out: bfloat16 [2048, 1024], P('ep', 'tp')
- moe_out: bfloat16 [4096, 2048], P(('ep', 'tp'))
The draws below stay inside these ranges and needn't reach their ends.
Inputs may be any that keep to these rules, and one draw needn't show every extreme that they name: `routes`: each row names 2 different experts. Within each aligned block of 128 rows no expert is named more than 64 times, and in every draw some expert is named exactly 64 times in some block.
All inputs are finite; a program needn't handle non-finite values.
Results may differ from the reference program's by a relative error of at most 0.012.
The reference program's roundings to bfloat16 on the way count: a program that leaves them out, or rounds other values in their place, can miss the bound.
Values may be sent and summed in bfloat16 or wider, within the bound.
A program may use at most 192 MiB of HBM per device.

```python
import math
import jax
import jax.numpy as jnp
import numpy as np
from jax import lax

D = 2048
HEADS = 16
KV_HEADS = 4
HD = 64
F = 1024
TOP = 2
GRID_W = 64
TOK_B = 128
TOKENS_A = 2048
TOKENS_B = 4096
EXPERTS = 8
CAP = 64
N_TP = 4


def draw_key_rows(key, part):
    result = jnp.clip(jax.random.normal(jax.random.fold_in(key, 72), (TOKENS_A, KV_HEADS * HD), jnp.float32), -6.0, 6.0)
    return result.astype(jnp.bfloat16)


def draw_query_rows(key, part):
    result = jnp.clip(jax.random.normal(jax.random.fold_in(key, 73), (TOKENS_A, HEADS * HD), jnp.float32), -6.0, 6.0)
    return result.astype(jnp.bfloat16)


def gain_draw(key, salt):
    result = jax.random.uniform(jax.random.fold_in(key, salt + 3), (HD,), jnp.float32, 1.2, 1.8)
    return result


def draw_query_gain(key, part):
    return gain_draw(key, 80)


def draw_key_gain(key, part):
    return gain_draw(key, 90)


def level_of(key, dims, pieces, low, top_value):
    factor_of, own = 1.0, jax.random.fold_in(key, 6)
    for axis_at, blocks in pieces:
        heights = jnp.exp(jax.random.uniform(jax.random.fold_in(own, axis_at), (blocks,), jnp.float32, low / len(pieces), top_value / len(pieces)))
        factor_of = factor_of * jnp.repeat(heights, dims[axis_at] // blocks).reshape([-1 if axis == axis_at else 1 for axis in range(len(dims))])
    return factor_of


def assign_block(stream_key, own, number, rows, amount, top, bound, slope):
    ranking = jax.random.permutation(stream_key, amount)
    crowded, common = portions_of(amount, rows * top, bound, slope, True), portions_of(amount, rows * top, bound, slope, False)
    places = jnp.arange(amount)

    def named(sizes, rotation):
        used = int((sizes > 0).sum())
        fixed = max(1, used // 4)
        passed = fixed + (places - fixed + rotation * (used - fixed)) % max(1, amount - fixed)
        return jnp.zeros((amount,), jnp.int32).at[ranking[jnp.where(places < fixed, places, passed)]].set(jnp.asarray(sizes, jnp.int32))

    sizes = jnp.where(number % 4 == 0, named(crowded, number // 4), named(common, number - number // 4 - 1))
    mixed = jax.random.permutation(jax.random.fold_in(own, 3), amount)
    source_of, receiver = mixed[0:amount // 2 * 2:2], mixed[1:amount // 2 * 2:2]
    room = jnp.minimum(sizes[source_of] - 1, bound - sizes[receiver]) // 2
    room = jnp.where((source_of == ranking[0]) | (receiver == ranking[0]) | (sizes[receiver] == 0), 0, jnp.maximum(room, 0))
    passed = jax.random.randint(jax.random.fold_in(own, 4), (amount // 2,), 0, 1 << 20) % (room + 1)
    sizes = sizes.at[source_of].add(-passed).at[receiver].add(passed)
    items = jnp.searchsorted(jnp.cumsum(sizes), jnp.arange(rows * top), side="right").astype(jnp.int32)
    table = items.reshape(top, rows).T
    table = table[jax.random.permutation(jax.random.fold_in(own, 1), rows)]
    rotation = jax.random.randint(jax.random.fold_in(own, 2), (rows, 1), 0, top)
    return jnp.take_along_axis(table, (jnp.arange(top)[None, :] + rotation) % top, axis=1)


def portions_of(number_of, total, limit, skew, full):
    weights = [(1 << 20) // math.isqrt(standing ** skew) + 1 for standing in range(1, number_of + 1)]
    largest = limit if full else min(limit, max(-(-total // number_of), total * weights[0] // sum(weights)))
    least = 1 if total - largest >= number_of - 1 else 0
    holding, surplus = [largest] + [least] * (number_of - 1), total - largest - least * (number_of - 1)
    while surplus > 0:
        movable = [i for i in range(1, number_of) if holding[i] < largest] or [i for i in range(1, number_of) if holding[i] < limit]
        pool, remaining = sum([weights[i] for i in movable]), surplus
        for i in movable:
            more = min(limit - holding[i], max(1, remaining * weights[i] // pool), surplus)
            holding[i] = holding[i] + more
            surplus = surplus - more
    return np.array(holding)


def gaussian(key, extent, width, reach, pieces=(), kind=jnp.bfloat16):
    entries = width * jax.random.normal(key, extent, jnp.float32)
    if pieces:
        entries = entries * level_of(key, extent, pieces, -0.22, 0.18)
    return jnp.clip(entries, -reach, reach).astype(kind)


def setup_inputs(seed: int = 0) -> dict:
    key_list = jax.random.split(jax.random.key(seed), 16)
    query_rows = draw_query_rows(jax.random.fold_in(key_list[15], 71), 0)
    key_rows = draw_key_rows(jax.random.fold_in(key_list[15], 71), 0)
    value_rows = gaussian(key_list[2], (TOKENS_A, KV_HEADS * HD), 3.0, 16.0, ((0, 8), (1, 4)))
    query_gain = draw_query_gain(jax.random.fold_in(key_list[15], 71), 0)
    key_gain = draw_key_gain(jax.random.fold_in(key_list[15], 71), 0)
    moe_tokens = gaussian(key_list[5], (TOKENS_B, D), 1.0, 6.0, ((0, 32),))
    norm_gain = jnp.clip(1.0 + 0.18 * jax.random.normal(key_list[6], (D,), jnp.float32), 0.1, 1.9)
    routes_keys = jax.random.split(jax.random.fold_in(key_list[7], 1), TOKENS_B // TOK_B)
    routes_turns = jax.random.permutation(jax.random.fold_in(key_list[7], 3), TOKENS_B // TOK_B)
    routes = jax.vmap(lambda own, number: assign_block(jax.random.fold_in(key_list[7], 2), own, number, TOK_B, EXPERTS, TOP, CAP, 1))(routes_keys, routes_turns).reshape((TOKENS_B, TOP))
    route_weights = jnp.clip(0.1 + 0.9 * jax.random.uniform(key_list[8], (TOKENS_B, TOP), jnp.float32) ** level_of(key_list[8], (TOKENS_B, TOP), ((0, 8),), -0.2, 0.2), 0.1, 1.0)
    expert_gate = gaussian(key_list[9], (EXPERTS, D, F), D ** -0.5, 0.125, ((0, 8), (2, 4)))
    expert_up = gaussian(key_list[10], (EXPERTS, D, F), D ** -0.5, 0.125, ((0, 8), (2, 4)))
    expert_down = gaussian(key_list[11], (EXPERTS, F, D), F ** -0.5, 0.1875, ((0, 8), (1, 4)))
    shared_gate = gaussian(key_list[12], (D, F), D ** -0.5, 0.125, ((1, 4),))
    shared_up = gaussian(key_list[13], (D, F), D ** -0.5, 0.125, ((1, 4),))
    shared_down = gaussian(key_list[14], (F, D), F ** -0.5, 0.1875, ((0, 4),))
    return {"query_rows": query_rows, "key_rows": key_rows, "value_rows": value_rows, "query_gain": query_gain, "key_gain": key_gain, "moe_tokens": moe_tokens, "norm_gain": norm_gain, "routes": routes, "route_weights": route_weights, "expert_gate": expert_gate, "expert_up": expert_up, "expert_down": expert_down, "shared_gate": shared_gate, "shared_up": shared_up, "shared_down": shared_down}


epsilon = 1e-06
rotary_base = 10000.0
routed_scale = 2.5

def rotate_heads(heads_in, gain_row, positions):
    values32 = heads_in.astype(jnp.float32)
    scaled = values32 * lax.rsqrt(lax.optimization_barrier(jnp.mean(values32 * values32, axis=-1, keepdims=True)) + epsilon) * gain_row
    pair_count = scaled.shape[-1] // 4
    inv_freq = rotary_base ** (-jnp.arange(pair_count, dtype=jnp.float32) / pair_count)
    grid_row = (positions // GRID_W).astype(jnp.float32)
    grid_col = (positions % GRID_W).astype(jnp.float32)
    angles = jnp.concatenate([grid_row[:, None] * inv_freq, grid_col[:, None] * inv_freq], axis=-1)[:, None, :]
    cosine = jnp.cos(angles)
    sine_part = jnp.sin(angles)
    first_half = scaled[..., 0::2]
    second_half = scaled[..., 1::2]
    turned = jnp.stack([first_half * cosine - second_half * sine_part, first_half * sine_part + second_half * cosine], axis=-1)
    return turned.reshape(scaled.shape).astype(jnp.bfloat16)

def attention(query_rows, key_rows, value_rows, query_gain, key_gain):
    token_count = query_rows.shape[0]
    group = HEADS // KV_HEADS
    positions = jnp.arange(token_count, dtype=jnp.int32)
    q_rot = rotate_heads(query_rows.reshape(token_count, HEADS, HD), query_gain, positions)
    k_rot = rotate_heads(key_rows.reshape(token_count, KV_HEADS, HD), key_gain, positions)
    keys32 = lax.optimization_barrier(k_rot).astype(jnp.float32)
    values32 = value_rows.reshape(token_count, KV_HEADS, HD).astype(jnp.float32)
    block_len = math.gcd(token_count, 256)
    q_blocks = lax.optimization_barrier(q_rot).reshape(token_count // block_len, block_len, KV_HEADS, group, HD)

    def one_block(q_block):
        scores = jnp.einsum('qgrd,sgd->qgrs', q_block.astype(jnp.float32), keys32) * HD ** (-0.5)
        row_max = lax.optimization_barrier(jnp.max(scores, axis=-1, keepdims=True))
        weights = jnp.exp(scores - row_max)
        row_sum = lax.optimization_barrier(jnp.sum(weights, axis=-1, keepdims=True))
        rounded = lax.optimization_barrier(weights.astype(jnp.bfloat16)).astype(jnp.float32)
        mixed = jnp.einsum('qgrs,sgd->qgrd', rounded, values32)
        return (mixed / row_sum).astype(jnp.bfloat16)
    result = lax.map(one_block, q_blocks)
    return result.reshape(token_count, HEADS * HD)

def feed_forward(rows_in, w_gate, w_up, w_down):
    gate_proj = jnp.dot(rows_in, w_gate, preferred_element_type=jnp.float32)
    up_proj = jnp.dot(rows_in, w_up, preferred_element_type=jnp.float32)
    hidden = lax.optimization_barrier((jax.nn.silu(gate_proj) * up_proj).astype(jnp.bfloat16))
    block_width = hidden.shape[-1] // N_TP
    summed = jnp.zeros((rows_in.shape[0], w_down.shape[1]), jnp.float32)
    for part_index in range(N_TP):
        lower = part_index * block_width
        partial_sum = jnp.dot(hidden[:, lower:lower + block_width], w_down[lower:lower + block_width], preferred_element_type=jnp.float32).astype(jnp.bfloat16)
        summed = summed + lax.optimization_barrier(partial_sum).astype(jnp.float32)
    return summed

def mixture(moe_tokens, norm_gain, routes, route_weights, expert_gate, expert_up, expert_down, shared_gate, shared_up, shared_down):
    total_rows = moe_tokens.shape[0]
    blocks = total_rows // TOK_B
    values32 = moe_tokens.astype(jnp.float32)
    normed = (values32 * lax.rsqrt(lax.optimization_barrier(jnp.mean(values32 * values32, axis=-1, keepdims=True)) + epsilon) * norm_gain).astype(jnp.bfloat16)
    normed = lax.optimization_barrier(normed)
    gates = route_weights / lax.optimization_barrier(jnp.sum(route_weights, axis=-1, keepdims=True)) * routed_scale
    chosen = routes.reshape(blocks, TOK_B * TOP).astype(jnp.int32)
    one_hot = (chosen[:, :, None] == jnp.arange(EXPERTS, dtype=jnp.int32)[None, None, :]).astype(jnp.int32)
    ranks = lax.optimization_barrier(jnp.sum((jnp.cumsum(one_hot, axis=1) - one_hot) * one_hot, axis=2))
    block_ids = jnp.arange(blocks, dtype=jnp.int32)[:, None]
    dest = (chosen * blocks + block_ids) * CAP + ranks
    rows_from = block_ids * TOK_B + jnp.arange(TOK_B * TOP, dtype=jnp.int32)[None, :] // TOP
    slot_rows = jnp.full((EXPERTS * blocks * CAP,), total_rows, jnp.int32).at[dest.reshape(-1)].set(rows_from.reshape(-1))
    padded = jnp.concatenate([normed, jnp.zeros((1, D), jnp.bfloat16)], axis=0)

    def one_expert(inputs):
        index_rows, w_gate, w_up, w_down = inputs
        return feed_forward(padded[index_rows], w_gate, w_up, w_down).astype(jnp.bfloat16)
    expert_rows = lax.map(one_expert, (slot_rows.reshape(EXPERTS, blocks * CAP), expert_gate, expert_up, expert_down))
    flat_rows = lax.optimization_barrier(expert_rows.reshape(EXPERTS * blocks * CAP, D))
    picked = flat_rows[dest.reshape(-1)].astype(jnp.float32).reshape(total_rows, TOP, D)
    routed = lax.optimization_barrier(jnp.sum(gates[:, :, None] * picked, axis=1))
    shared = feed_forward(normed, shared_gate, shared_up, shared_down)
    return (routed + shared).astype(jnp.bfloat16)

def reference(query_rows, key_rows, value_rows, query_gain, key_gain, moe_tokens, norm_gain, routes, route_weights, expert_gate, expert_up, expert_down, shared_gate, shared_up, shared_down):
    attn_out = attention(query_rows, key_rows, value_rows, query_gain, key_gain)
    moe_out = mixture(moe_tokens, norm_gain, routes, route_weights, expert_gate, expert_up, expert_down, shared_gate, shared_up, shared_down)
    return (attn_out, moe_out)
```

```python
import functools
import math

import jax
import jax.numpy as jnp
from jax import lax
from jax.experimental import pallas as pl
from jax.experimental.pallas import tpu as pltpu
from jax.sharding import PartitionSpec as P

GRID_W = 64
MESH = pl.DeviceIdType.MESH


epsilon = 1e-06
rotary_base = 10000.0
routed_scale = 2.5


def flip(number, mask):
    result, bit = number, 1
    while bit <= mask:
        if mask & bit:
            result = result + bit - 2 * bit * lax.rem(lax.div(number, bit), 2)
        bit *= 2
    return result


def doubled(blocks, axis):
    n = lax.axis_size(axis)
    masks, step = [0], n // 2
    while step:
        pairs = [(j, j ^ step) for j in range(n)]
        blocks = blocks + [lax.ppermute(block, axis, pairs) for block in blocks]
        masks = masks + [mask ^ step for mask in masks]
        step //= 2
    return blocks, masks


def each_peer(axis, sizes, step):
    if axis == "tp":
        for i in range(1, sizes[axis]):
            step(i, 0)
    else:
        lax.fori_loop(1, sizes[axis], step, 0)


def exchange_kernel(plan, sizes, *refs):
    count = len(plan)
    sources, targets = refs[:count], refs[count : 2 * count]
    send_sems = refs[2 * count : 3 * count]
    recv_sems = refs[3 * count : 4 * count]
    own_sems = refs[4 * count]
    axes = []
    for axis, _ in plan:
        if axis not in axes:
            axes.append(axis)
    barrier = pltpu.get_barrier_semaphore()
    for axis in axes:
        me, n = lax.axis_index(axis), sizes[axis]

        def greet(i, c, axis=axis, me=me, n=n):
            pl.semaphore_signal(
                barrier, inc=1, device_id={axis: lax.rem(me + i, n)}, device_id_type=MESH
            )
            return c

        lax.fori_loop(1, n, greet, 0)
    pl.semaphore_wait(barrier, sum(sizes[axis] - 1 for axis in axes))

    def copy_of(k, i):
        axis, scattered = plan[k]
        me, n = lax.axis_index(axis), sizes[axis]
        if axis == "tp":
            peer, source_at, target_at = flip(me, i), i, i
        else:
            peer = lax.rem(me + i, n)
            source_at, target_at = peer, me
        return pltpu.make_async_remote_copy(
            src_ref=sources[k].at[source_at] if scattered else sources[k],
            dst_ref=targets[k].at[target_at],
            send_sem=send_sems[k].at[i],
            recv_sem=recv_sems[k].at[i],
            device_id={axis: peer},
            device_id_type=MESH,
        )

    for k, (axis, scattered) in enumerate(plan):

        def begin(i, c, k=k):
            copy_of(k, i).start()
            return c

        each_peer(axis, sizes, begin)
    local = []
    for k, (axis, scattered) in enumerate(plan):
        me = 0 if axis == "tp" else lax.axis_index(axis)
        copy = pltpu.make_async_copy(
            sources[k].at[me] if scattered else sources[k], targets[k].at[me], own_sems.at[k]
        )
        copy.start()
        local.append(copy)
    for copy in local:
        copy.wait()
    for k, (axis, scattered) in enumerate(plan):

        def finish(i, c, k=k):
            copy_of(k, i).wait()
            return c

        each_peer(axis, sizes, finish)


def exchange(operands, plan, number):
    sizes = {axis: lax.axis_size(axis) for axis, _ in plan}
    shapes = []
    for array, (axis, scattered) in zip(operands, plan):
        shape = array.shape if scattered else (sizes[axis],) + array.shape
        shapes.append(jax.ShapeDtypeStruct(shape, array.dtype))
    sems = [pltpu.SemaphoreType.DMA((sizes[axis],)) for axis, _ in plan]
    traffic = 2 * sum(s.size * s.dtype.itemsize for s in shapes)
    return pl.pallas_call(
        functools.partial(exchange_kernel, plan, sizes),
        out_shape=shapes,
        in_specs=[pl.BlockSpec(memory_space=pl.ANY)] * len(plan),
        out_specs=[pl.BlockSpec(memory_space=pl.ANY)] * len(plan),
        scratch_shapes=sems + sems + [pltpu.SemaphoreType.DMA((len(plan),))],
        compiler_params=pltpu.CompilerParams(collective_id=number, has_side_effects=True),
        cost_estimate=pl.CostEstimate(
            flops=0, bytes_accessed=16 * traffic, transcendentals=0
        ),
    )(*operands)


def rotate_heads(heads_in, gain_row, positions):
    values32 = heads_in.astype(jnp.float32)
    scaled = (
        values32
        * lax.rsqrt(jnp.mean(values32 * values32, axis=-1, keepdims=True) + epsilon)
        * gain_row
    )
    pair_count = scaled.shape[-1] // 4
    inv_freq = rotary_base ** (-jnp.arange(pair_count, dtype=jnp.float32) / pair_count)
    grid_row = (positions // GRID_W).astype(jnp.float32)
    grid_col = (positions % GRID_W).astype(jnp.float32)
    angles = jnp.concatenate([grid_row[:, None] * inv_freq, grid_col[:, None] * inv_freq], axis=-1)[
        :, None, :
    ]
    cosine = jnp.cos(angles)
    sine_part = jnp.sin(angles)
    first_half = scaled[..., 0::2]
    second_half = scaled[..., 1::2]
    turned = jnp.stack(
        [
            first_half * cosine - second_half * sine_part,
            first_half * sine_part + second_half * cosine,
        ],
        axis=-1,
    )
    return turned.reshape(scaled.shape).astype(jnp.bfloat16)


def span_length(row_count):
    length = min(row_count, 2048)
    while row_count % length:
        length -= 1
    return length


def rotated(query_rows, key_rows, value_rows, query_gain, key_gain):
    row_count = query_rows.shape[0]
    head_size = query_gain.shape[0]
    q_heads = query_rows.shape[1] // head_size
    kv_heads = key_rows.shape[1] // head_size
    positions = lax.axis_index("ep") * row_count + jnp.arange(row_count, dtype=jnp.int32)
    q_rot = rotate_heads(query_rows.reshape(row_count, q_heads, head_size), query_gain, positions)
    k_rot = rotate_heads(key_rows.reshape(row_count, kv_heads, head_size), key_gain, positions)
    key_value = jnp.stack([k_rot, value_rows.reshape(row_count, kv_heads, head_size)], axis=2)
    return q_rot, key_value.reshape(row_count, kv_heads * 2 * head_size)


def attend(q_rot, piece_rows):
    row_count, q_heads, head_size = q_rot.shape
    kv_heads = piece_rows.shape[1] // (2 * head_size)
    group = q_heads // kv_heads
    scale = head_size ** (-0.5)
    q_grouped = q_rot.reshape(row_count, kv_heads, group, head_size).transpose(1, 2, 0, 3)
    q_grouped = q_grouped.reshape(kv_heads, group * row_count, head_size)
    query_count = group * row_count
    initial = (
        jnp.full((kv_heads, query_count), -jnp.inf, jnp.float32),
        jnp.zeros((kv_heads, query_count), jnp.float32),
        jnp.zeros((kv_heads, query_count, head_size), jnp.float32),
    )

    def one_span(carried, span_rows):
        run_max, run_sum, mixed = carried
        keys_span = span_rows[:, :, 0, :]
        values_span = span_rows[:, :, 1, :]
        scores = (
            jnp.einsum("hrd,shd->hrs", q_grouped, keys_span, preferred_element_type=jnp.float32)
            * scale
        )
        new_max = jnp.maximum(run_max, jnp.max(scores, axis=-1))
        factor = jnp.exp(run_max - new_max)
        weights = jnp.exp(scores - new_max[..., None])
        run_sum = run_sum * factor + jnp.sum(weights, axis=-1)
        added = jnp.einsum(
            "hrs,shd->hrd",
            weights.astype(jnp.bfloat16),
            values_span,
            preferred_element_type=jnp.float32,
        )
        mixed = mixed * factor[..., None] + added
        return ((new_max, run_sum, mixed), None)

    piece_count = piece_rows.shape[0]
    length = span_length(piece_count)
    spans = piece_rows.reshape(piece_count // length, length, kv_heads, 2, head_size)
    carried, unused = lax.scan(one_span, initial, spans)
    run_max, run_sum, mixed = carried
    result = (mixed / run_sum[..., None]).astype(jnp.bfloat16)
    result = result.reshape(kv_heads, group, row_count, head_size).transpose(2, 0, 1, 3)
    return result.reshape(row_count, q_heads * head_size)


def slot_numbers(own_routes, experts, capacity):
    tok_rows = own_routes.shape[0]
    named = own_routes[:, :, None] == jnp.arange(experts, dtype=jnp.int32)
    counts = jnp.any(named, axis=1).astype(jnp.bfloat16)
    rows = jnp.arange(tok_rows, dtype=jnp.int32)
    before = (rows[:, None] > rows[None, :]).astype(jnp.bfloat16)
    earlier = jnp.dot(before, counts, preferred_element_type=jnp.float32)
    ranks = jnp.sum(jnp.where(named, earlier[:, None, :], 0.0), axis=2).astype(jnp.int32)
    return own_routes * capacity + ranks


def hidden_of(rows_in, w_gate, w_up):
    gate_proj = jnp.einsum("...rd,...df->...rf", rows_in, w_gate, preferred_element_type=jnp.float32)
    up_proj = jnp.einsum("...rd,...df->...rf", rows_in, w_up, preferred_element_type=jnp.float32)
    return lax.optimization_barrier((jax.nn.silu(gate_proj) * up_proj).astype(jnp.bfloat16))


def plain_body(
    query_rows,
    key_rows,
    value_rows,
    query_gain,
    key_gain,
    moe_tokens,
    norm_gain,
    routes,
    route_weights,
    expert_gate,
    expert_up,
    expert_down,
    shared_gate,
    shared_up,
    shared_down,
):
    tok_rows, model_width = moe_tokens.shape
    top_count = routes.shape[1]
    tp_size = lax.axis_size("tp")
    ep_size = lax.axis_size("ep")
    local_experts = expert_gate.shape[0]
    experts = local_experts * ep_size
    capacity = 2 * tok_rows * top_count // experts
    lane = lax.axis_index("tp")

    all_gate, _ = doubled([expert_gate], "tp")
    all_up, _ = doubled([expert_up], "tp")
    all_down, _ = doubled([expert_down], "tp")

    values32 = moe_tokens.astype(jnp.float32)
    normed = (
        values32
        * lax.rsqrt(jnp.mean(values32 * values32, axis=-1, keepdims=True) + epsilon)
        * norm_gain
    ).astype(jnp.bfloat16)
    own_routes = lax.dynamic_slice_in_dim(routes, lane * tok_rows, tok_rows, 0)
    own_weights = lax.dynamic_slice_in_dim(route_weights, lane * tok_rows, tok_rows, 0)
    own_gates = own_weights / jnp.sum(own_weights, axis=-1, keepdims=True) * routed_scale
    slots = slot_numbers(own_routes, experts, capacity)
    slot_ids = jnp.arange(experts * capacity, dtype=jnp.int32)
    placing = jnp.any(slot_ids[:, None, None] == slots[None, :, :], axis=2).astype(jnp.bfloat16)
    send = jnp.dot(placing, normed, preferred_element_type=jnp.float32).astype(jnp.bfloat16)
    send = send.reshape(ep_size, local_experts * capacity, model_width)

    q_rot, key_value = rotated(query_rows, key_rows, value_rows, query_gain, key_gain)

    group_rows, masks = doubled([normed], "tp")
    arrived, pieces = exchange((send, key_value), (("ep", True), ("ep", False)), 1)
    attn_out = attend(q_rot, pieces.reshape(-1, pieces.shape[-1]))
    group_rows = jnp.concatenate([group_rows[masks.index(i)] for i in range(tp_size)], axis=0)
    shared_hidden = hidden_of(group_rows, shared_gate, shared_up)
    shared_part = jnp.dot(shared_hidden, shared_down, preferred_element_type=jnp.float32)
    shared_part = shared_part.astype(jnp.bfloat16).reshape(tp_size, tok_rows, model_width)

    arrived = arrived.reshape(ep_size, local_experts, capacity, model_width).transpose(1, 0, 2, 3)
    arrived = arrived.reshape(local_experts, ep_size * capacity, model_width)
    total = 0.0
    for part in range(tp_size):
        hidden = hidden_of(arrived, all_gate[part], all_up[part])
        partial = jnp.einsum(
            "lrf,lfd->lrd", hidden, all_down[part], preferred_element_type=jnp.float32
        )
        total = total + partial.astype(jnp.bfloat16).astype(jnp.float32)
    outgoing = total.astype(jnp.bfloat16).reshape(local_experts, ep_size, capacity, model_width)
    outgoing = outgoing.transpose(1, 0, 2, 3).reshape(
        ep_size, local_experts * capacity, model_width
    )
    returned, shared_parts = exchange((outgoing, shared_part), (("ep", True), ("tp", True)), 2)

    flat_rows = returned.reshape(experts * capacity, model_width)
    moe_out = jnp.sum(shared_parts.astype(jnp.float32), axis=0)
    for k in range(top_count):
        choosing = (slots[:, k, None] == slot_ids[None, :]).astype(jnp.bfloat16)
        picked = jnp.dot(choosing, flat_rows, preferred_element_type=jnp.float32)
        moe_out = moe_out + own_gates[:, k, None] * picked
    return (attn_out, moe_out.astype(jnp.bfloat16))


PARTS = 4
CHUNKS = 4


def fused_kernel(
    sizes,
    slots_t_ref,
    slots_ref,
    gates_ref,
    normed_ref,
    q_ref,
    k_ref,
    v_ref,
    q_gain_ref,
    k_gain_ref,
    cos_ref,
    sin_ref,
    gate_hbm,
    up_hbm,
    down_hbm,
    sgate_hbm,
    sup_hbm,
    sdown_hbm,
    attn_ref,
    moe_ref,
    w_gate,
    w_up,
    w_down,
    s_gate,
    s_up,
    s_down,
    send,
    arrived,
    outgoing,
    returned,
    hidden,
    gate_acc,
    s_hidden,
    pieces,
    q_rot,
    other_rows,
    part_out,
    part_in,
    total,
    load_sems,
    core_sems,
    y_sems,
    relay_sems,
    slot_sems,
    kv_sems,
    back_sems,
):
    n_ep, capacity = sizes
    me, lane = lax.axis_index("ep"), lax.axis_index("tp")
    core, across = {"tp": flip(lane, 1)}, {"tp": flip(lane, 2)}
    rows, width = normed_ref.shape
    chunk = width // CHUNKS
    bf16, f32 = jnp.bfloat16, jnp.float32

    def remote(source, target, sems, i, device):
        return pltpu.make_async_remote_copy(
            src_ref=source,
            dst_ref=target,
            send_sem=sems.at[(0,) + i],
            recv_sem=sems.at[(1,) + i],
            device_id=device,
            device_id_type=MESH,
        )

    def columns(q):
        return pl.ds(q * chunk, chunk)

    own = [
        (gate_hbm.at[0], w_gate),
        (up_hbm.at[0], w_up),
        (down_hbm.at[0], w_down),
        (sgate_hbm, s_gate),
        (sup_hbm, s_up),
        (sdown_hbm, s_down),
    ]
    loads = [
        pltpu.make_async_copy(source, target.at[0], load_sems.at[j])
        for j, (source, target) in enumerate(own)
    ]
    to_core = [
        remote(source, target.at[1], core_sems, (j,), core)
        for j, (source, target) in enumerate(own)
    ]
    down_pieces = [
        (down_hbm.at[0, :, columns(q)], w_down.at[2, :, columns(q)]) for q in range(CHUNKS)
    ]
    to_across = [
        remote(source, target, y_sems, (j,), across)
        for j, (source, target) in enumerate(
            [(gate_hbm.at[0], w_gate.at[2]), (up_hbm.at[0], w_up.at[2])]
            + down_pieces
            + [(normed_ref, other_rows), (part_out, part_in)]
        )
    ]
    relayed = [
        remote(source, target, relay_sems, (j,), core)
        for j, (source, target) in enumerate(
            [(w_gate.at[2], w_gate.at[3]), (w_up.at[2], w_up.at[3])]
            + [(w_down.at[2, :, columns(q)], w_down.at[3, :, columns(q)]) for q in range(CHUNKS)]
        )
    ]

    def slots_to(i):
        return remote(send.at[i], arrived.at[i], slot_sems, (i,), {"ep": flip(me, i)})

    def pieces_to(i):
        return remote(pieces.at[me], pieces.at[me], kv_sems, (i,), {"ep": flip(me, i)})

    def back_to(q, i):
        return remote(
            outgoing.at[i, :, columns(q)],
            returned.at[me, :, columns(q)],
            back_sems,
            (q, i),
            {"ep": flip(me, i)},
        )

    def place(i):
        base = flip(me, i) * capacity
        index = lax.broadcasted_iota(jnp.int32, (capacity, rows), 0) + base
        chosen = index == slots_t_ref[0:1, :]
        for k in range(1, slots_t_ref.shape[0]):
            chosen = chosen | (index == slots_t_ref[k : k + 1, :])
        chosen = jnp.where(chosen, 1.0, 0.0).astype(bf16)
        packed = jnp.dot(chosen, normed_ref[...], preferred_element_type=f32).astype(bf16)
        if i:
            send[i] = packed
        else:
            arrived[0] = packed

    barrier = pltpu.get_barrier_semaphore()
    for device in [core, across] + [{"ep": flip(me, i)} for i in range(1, n_ep)]:
        pl.semaphore_signal(barrier, inc=1, device_id=device, device_id_type=MESH)
    for load in loads:
        load.start()
    order = list(range(1, n_ep))
    place(order[0])
    place(order[1])
    pl.semaphore_wait(barrier, n_ep + 1)
    for copy in to_across[:2] + to_core:
        copy.start()
    for at in range(len(order)):
        slots_to(order[at]).start()
        if at + 2 < len(order):
            place(order[at + 2])
    place(0)

    head = q_gain_ref.shape[1]
    q_heads = q_ref.shape[1] // head

    def turned(values, factor, cosine, sine):
        scaled = values * factor
        span = values.shape[1]
        even = lax.broadcasted_iota(jnp.int32, values.shape, 1) % 2 == 0
        swapped = jnp.where(even, pltpu.roll(scaled, span - 1, 1), pltpu.roll(scaled, 1, 1))
        return scaled * cosine + swapped * sine

    def factor_of(values):
        return lax.rsqrt(jnp.mean(values * values, axis=-1, keepdims=True) + epsilon)

    key32 = k_ref[...].astype(f32)
    key32 = key32 * factor_of(key32) * k_gain_ref[...]
    value32 = v_ref[...].astype(f32)
    joined = jnp.concatenate([key32, value32], axis=1)
    in_key = lax.broadcasted_iota(jnp.int32, joined.shape, 1) < head
    spun = turned(joined, 1.0, cos_ref[...], sin_ref[...])
    pieces[me] = jnp.where(in_key, spun, joined).astype(bf16)
    scale = head ** (-0.5)
    for h in range(0, q_heads, 2):
        pair = [q_ref[:, (h + j) * head : (h + j + 1) * head].astype(f32) for j in range(2)]
        pair = [x * factor_of(x) * q_gain_ref[...] for x in pair]
        spun = turned(jnp.concatenate(pair, axis=1), 1.0, cos_ref[...], sin_ref[...])
        spun = spun.astype(bf16) * jnp.asarray(scale, bf16)
        zero = jnp.zeros((spun.shape[0], head), bf16)
        for j in range(2):
            q_rot[h + j] = jnp.concatenate([spun[:, j * head : (j + 1) * head], zero], axis=1)
    for i in range(1, n_ep):
        pieces_to(i).start()

    half = n_ep // 2
    group_rows = half * capacity

    def rows_of(g):
        return arrived[g * half : (g + 1) * half].reshape(group_rows, width)

    def span_of(g):
        return pl.ds(g * group_rows, group_rows)

    def gate_of(p, g):
        gate_acc[p, span_of(g), :] = jnp.dot(rows_of(g), w_gate[p], preferred_element_type=f32)

    def hidden_at(p, g):
        up_proj = jnp.dot(rows_of(g), w_up[p], preferred_element_type=f32)
        gate_proj = gate_acc[p, span_of(g), :]
        hidden[p, span_of(g), :] = (jax.nn.silu(gate_proj) * up_proj).astype(bf16)

    for i in range(1, half):
        slots_to(i).wait_recv()
    for load in loads:
        load.wait()
    gate_of(0, 0)
    hidden_at(0, 0)
    for copy in to_core:
        copy.wait()
    gate_of(1, 0)
    hidden_at(1, 0)
    to_across[0].wait()
    relayed[0].start()
    for copy in to_across[2 : 3 + CHUNKS]:
        copy.start()
    gate_of(2, 0)
    relayed[0].wait()
    gate_of(3, 0)
    for i in range(half, n_ep):
        slots_to(i).wait_recv()
    gate_of(0, 1)
    hidden_at(0, 1)
    gate_of(1, 1)
    hidden_at(1, 1)
    gate_of(2, 1)
    gate_of(3, 1)
    to_across[1].wait()
    relayed[1].start()
    for g in range(2):
        hidden_at(2, g)
    relayed[1].wait()
    for g in range(2):
        hidden_at(3, g)

    for q in range(CHUNKS):
        to_across[2 + q].wait()
        relayed[2 + q].start()
        relayed[2 + q].wait()
        for g in range(2):
            summed = 0.0
            for p in range(PARTS):
                partial = jnp.dot(
                    hidden[p, span_of(g), :], w_down[p, :, columns(q)], preferred_element_type=f32
                )
                summed = summed + partial.astype(bf16).astype(f32)
            outgoing[g * half : (g + 1) * half, :, columns(q)] = summed.astype(bf16).reshape(
                half, capacity, chunk
            )
        returned[me, :, columns(q)] = outgoing[0, :, columns(q)]
        for i in range(1, n_ep):
            back_to(q, i).start()

    def shared_hidden(source, p):
        gate_proj = jnp.dot(source[...], s_gate[p], preferred_element_type=f32)
        up_proj = jnp.dot(source[...], s_up[p], preferred_element_type=f32)
        s_hidden[p] = (jax.nn.silu(gate_proj) * up_proj).astype(bf16)

    def shared_down(q):
        summed = 0.0
        for p in range(2):
            partial = jnp.dot(s_hidden[p], s_down[p, :, columns(q)], preferred_element_type=f32)
            summed = summed + partial.astype(bf16).astype(f32)
        return summed

    to_across[2 + CHUNKS].wait()
    for p in range(2):
        shared_hidden(other_rows, p)
    for q in range(CHUNKS):
        part_out[:, columns(q)] = shared_down(q).astype(bf16)
    for p in range(2):
        shared_hidden(normed_ref, p)
    to_across[3 + CHUNKS].start()
    for q in range(CHUNKS):
        total[:, columns(q)] = shared_down(q)

    for i in range(1, n_ep):
        pieces_to(i).wait()
    row_count = q_ref.shape[0]
    block = 128
    keys = pieces[...].reshape(n_ep * row_count, 2 * head)

    for h in range(q_heads):

        def one_block(b, c, h=h):
            at = pl.ds(pl.multiple_of(b * block, block), block)
            scores = lax.dot_general(
                q_rot[h, at, :],
                pieces[...].reshape(n_ep * row_count, 2 * head),
                (((1,), (1,)), ((), ())),
                preferred_element_type=f32,
            )
            weights = jnp.exp(scores - jnp.max(scores, axis=-1, keepdims=True))
            row_sum = jnp.sum(weights, axis=-1, keepdims=True)
            mixed = jnp.dot(
                weights.astype(bf16),
                pieces[...].reshape(n_ep * row_count, 2 * head),
                preferred_element_type=f32,
            )
            attn_ref[at, h * head : (h + 1) * head] = (mixed / row_sum)[:, head:].astype(bf16)
            return c

        lax.fori_loop(0, row_count // block, one_block, 0)

    index = lax.broadcasted_iota(jnp.int32, (rows, n_ep * capacity), 1)
    choosing = [
        jnp.where(index == slots_ref[:, k : k + 1], 1.0, 0.0).astype(bf16)
        for k in range(slots_ref.shape[1])
    ]
    to_across[3 + CHUNKS].wait()
    for i in range(1, n_ep):
        slots_to(i).wait_send()
    for q in range(CHUNKS):
        for i in range(1, n_ep):
            back_to(q, i).wait()
        flat = returned[:, :, columns(q)].reshape(n_ep * capacity, chunk)
        summed = total[:, columns(q)] + part_in[:, columns(q)].astype(f32)
        for k, chosen in enumerate(choosing):
            picked = jnp.dot(chosen, flat, preferred_element_type=f32)
            summed = summed + gates_ref[:, k : k + 1] * picked
        moe_ref[:, columns(q)] = summed.astype(bf16)


def fused_body(
    query_rows,
    key_rows,
    value_rows,
    query_gain,
    key_gain,
    moe_tokens,
    norm_gain,
    routes,
    route_weights,
    expert_gate,
    expert_up,
    expert_down,
    shared_gate,
    shared_up,
    shared_down,
):
    tok_rows, model_width = moe_tokens.shape
    row_count = query_rows.shape[0]
    head_size = query_gain.shape[0]
    top_count = routes.shape[1]
    ep_size = lax.axis_size("ep")
    experts = ep_size
    capacity = 2 * tok_rows * top_count // experts
    units = expert_gate.shape[2]
    lane = lax.axis_index("tp")

    values32 = moe_tokens.astype(jnp.float32)
    normed = (
        values32
        * lax.rsqrt(jnp.mean(values32 * values32, axis=-1, keepdims=True) + epsilon)
        * norm_gain
    ).astype(jnp.bfloat16)
    own_routes = lax.dynamic_slice_in_dim(routes, lane * tok_rows, tok_rows, 0)
    own_weights = lax.dynamic_slice_in_dim(route_weights, lane * tok_rows, tok_rows, 0)
    own_gates = own_weights / jnp.sum(own_weights, axis=-1, keepdims=True) * routed_scale
    slots = slot_numbers(own_routes, experts, capacity)

    positions = lax.axis_index("ep") * row_count + jnp.arange(row_count, dtype=jnp.int32)
    pair_count = head_size // 4
    pair = (jnp.arange(2 * head_size, dtype=jnp.int32) % head_size) // 2
    inv_freq = rotary_base ** (-(pair % pair_count).astype(jnp.float32) / pair_count)
    grid_row = (positions // GRID_W).astype(jnp.float32)
    grid_col = (positions % GRID_W).astype(jnp.float32)
    angles = jnp.where(pair < pair_count, grid_row[:, None], grid_col[:, None]) * inv_freq
    sign = jnp.where(jnp.arange(2 * head_size) % 2 == 0, -1.0, 1.0).astype(jnp.float32)
    cosine = jnp.cos(angles)
    sine = jnp.sin(angles) * sign

    bf16, f32 = jnp.bfloat16, jnp.float32
    vmem, anywhere = pl.BlockSpec(memory_space=pltpu.VMEM), pl.BlockSpec(memory_space=pl.ANY)
    dma = pltpu.SemaphoreType.DMA
    slot_shape = (ep_size, capacity, model_width)
    all_rows = ep_size * capacity
    return pl.pallas_call(
        functools.partial(fused_kernel, (ep_size, capacity)),
        out_shape=[
            jax.ShapeDtypeStruct(query_rows.shape, bf16),
            jax.ShapeDtypeStruct(moe_tokens.shape, bf16),
        ],
        in_specs=[vmem] * 11 + [anywhere] * 6,
        out_specs=[vmem] * 2,
        scratch_shapes=[
            pltpu.VMEM((PARTS, model_width, units), bf16),
            pltpu.VMEM((PARTS, model_width, units), bf16),
            pltpu.VMEM((PARTS, units, model_width), bf16),
            pltpu.VMEM((2, model_width, units), bf16),
            pltpu.VMEM((2, model_width, units), bf16),
            pltpu.VMEM((2, units, model_width), bf16),
            pltpu.VMEM(slot_shape, bf16),
            pltpu.VMEM(slot_shape, bf16),
            pltpu.VMEM(slot_shape, bf16),
            pltpu.VMEM(slot_shape, bf16),
            pltpu.VMEM((PARTS, all_rows, units), bf16),
            pltpu.VMEM((PARTS, all_rows, units), f32),
            pltpu.VMEM((2, tok_rows, units), bf16),
            pltpu.VMEM((ep_size, row_count, 2 * head_size), bf16),
            pltpu.VMEM((query_rows.shape[1] // head_size, row_count, 2 * head_size), bf16),
            pltpu.VMEM((tok_rows, model_width), bf16),
            pltpu.VMEM((tok_rows, model_width), bf16),
            pltpu.VMEM((tok_rows, model_width), bf16),
            pltpu.VMEM((tok_rows, model_width), f32),
            dma((6,)),
            dma((2, 6)),
            dma((2, 4 + CHUNKS)),
            dma((2, 2 + CHUNKS)),
            dma((2, ep_size)),
            dma((2, ep_size)),
            dma((2, CHUNKS, ep_size)),
        ],
        compiler_params=pltpu.CompilerParams(
            collective_id=3, has_side_effects=True, vmem_limit_bytes=60 * 1024 * 1024
        ),
    )(
        slots.T,
        slots,
        own_gates,
        normed,
        query_rows,
        key_rows,
        value_rows,
        query_gain[None],
        key_gain[None],
        cosine,
        sine,
        expert_gate,
        expert_up,
        expert_down,
        shared_gate,
        shared_up,
        shared_down,
    )


def body(*arrays):
    query_rows, query_gain, moe_tokens, routes = arrays[0], arrays[3], arrays[5], arrays[7]
    expert_gate = arrays[9]
    ep_size, tp_size = lax.axis_size("ep"), lax.axis_size("tp")
    capacity = 2 * moe_tokens.shape[0] * routes.shape[1] // (ep_size * expert_gate.shape[0])
    head_size = query_gain.shape[0]
    one_kernel = (
        tp_size == PARTS
        and expert_gate.shape[0] == 1
        and ep_size & (ep_size - 1) == 0
        and capacity % 16 == 0
        and ep_size * query_rows.shape[0] * 2 * head_size <= 1 << 20
        and query_rows.shape[1] // head_size % 2 == 0
        and arrays[1].shape[1] == head_size
        and 2 * head_size % 128 == 0
        and math.log2(head_size) % 2 == 0
    )
    return fused_body(*arrays) if one_kernel else plain_body(*arrays)


def solution(mesh):
    return jax.shard_map(
        body,
        mesh=mesh,
        in_specs=(
            P("ep", "tp"),
            P("ep", "tp"),
            P("ep", "tp"),
            P(),
            P(),
            P(("ep", "tp"), None),
            P(),
            P("ep", None),
            P("ep", None),
            P("ep", None, "tp"),
            P("ep", None, "tp"),
            P("ep", "tp", None),
            P(None, "tp"),
            P(None, "tp"),
            P("tp", None),
        ),
        out_specs=(P("ep", "tp"), P(("ep", "tp"), None)),
        check_vma=False,
    )
```

```python
import functools
import math

import jax
import jax.numpy as jnp
import numpy as np
from jax import lax
from jax.experimental import pallas as pl
from jax.experimental.pallas import tpu as pltpu
from jax.sharding import PartitionSpec as P

GRID_W = 64
MESH = pl.DeviceIdType.MESH


epsilon = 1e-06
rotary_base = 10000.0
routed_scale = 2.5


def flip(number, mask):
    result, bit = number, 1
    while bit <= mask:
        if mask & bit:
            result = result + bit - 2 * bit * lax.rem(lax.div(number, bit), 2)
        bit *= 2
    return result


def doubled(blocks, axis):
    n = lax.axis_size(axis)
    masks, step = [0], n // 2
    while step:
        pairs = [(j, j ^ step) for j in range(n)]
        blocks = blocks + [lax.ppermute(block, axis, pairs) for block in blocks]
        masks = masks + [mask ^ step for mask in masks]
        step //= 2
    return blocks, masks


def each_peer(axis, sizes, step):
    if axis == "tp":
        for i in range(1, sizes[axis]):
            step(i, 0)
    else:
        lax.fori_loop(1, sizes[axis], step, 0)


def exchange_kernel(plan, sizes, *refs):
    count = len(plan)
    sources, targets = refs[:count], refs[count : 2 * count]
    send_sems = refs[2 * count : 3 * count]
    recv_sems = refs[3 * count : 4 * count]
    own_sems = refs[4 * count]
    axes = []
    for axis, _ in plan:
        if axis not in axes:
            axes.append(axis)
    barrier = pltpu.get_barrier_semaphore()
    for axis in axes:
        me, n = lax.axis_index(axis), sizes[axis]

        def greet(i, c, axis=axis, me=me, n=n):
            pl.semaphore_signal(
                barrier, inc=1, device_id={axis: lax.rem(me + i, n)}, device_id_type=MESH
            )
            return c

        lax.fori_loop(1, n, greet, 0)
    pl.semaphore_wait(barrier, sum(sizes[axis] - 1 for axis in axes))

    def copy_of(k, i):
        axis, scattered = plan[k]
        me, n = lax.axis_index(axis), sizes[axis]
        if axis == "tp":
            peer, source_at, target_at = flip(me, i), i, i
        else:
            peer = lax.rem(me + i, n)
            source_at, target_at = peer, me
        return pltpu.make_async_remote_copy(
            src_ref=sources[k].at[source_at] if scattered else sources[k],
            dst_ref=targets[k].at[target_at],
            send_sem=send_sems[k].at[i],
            recv_sem=recv_sems[k].at[i],
            device_id={axis: peer},
            device_id_type=MESH,
        )

    for k, (axis, scattered) in enumerate(plan):

        def begin(i, c, k=k):
            copy_of(k, i).start()
            return c

        each_peer(axis, sizes, begin)
    local = []
    for k, (axis, scattered) in enumerate(plan):
        me = 0 if axis == "tp" else lax.axis_index(axis)
        copy = pltpu.make_async_copy(
            sources[k].at[me] if scattered else sources[k], targets[k].at[me], own_sems.at[k]
        )
        copy.start()
        local.append(copy)
    for copy in local:
        copy.wait()
    for k, (axis, scattered) in enumerate(plan):

        def finish(i, c, k=k):
            copy_of(k, i).wait()
            return c

        each_peer(axis, sizes, finish)


def exchange(operands, plan, number):
    sizes = {axis: lax.axis_size(axis) for axis, _ in plan}
    shapes = []
    for array, (axis, scattered) in zip(operands, plan):
        shape = array.shape if scattered else (sizes[axis],) + array.shape
        shapes.append(jax.ShapeDtypeStruct(shape, array.dtype))
    sems = [pltpu.SemaphoreType.DMA((sizes[axis],)) for axis, _ in plan]
    traffic = 2 * sum(s.size * s.dtype.itemsize for s in shapes)
    return pl.pallas_call(
        functools.partial(exchange_kernel, plan, sizes),
        out_shape=shapes,
        in_specs=[pl.BlockSpec(memory_space=pl.ANY)] * len(plan),
        out_specs=[pl.BlockSpec(memory_space=pl.ANY)] * len(plan),
        scratch_shapes=sems + sems + [pltpu.SemaphoreType.DMA((len(plan),))],
        compiler_params=pltpu.CompilerParams(collective_id=number, has_side_effects=True),
        cost_estimate=pl.CostEstimate(
            flops=0, bytes_accessed=16 * traffic, transcendentals=0
        ),
    )(*operands)


def rotate_heads(heads_in, gain_row, positions):
    values32 = heads_in.astype(jnp.float32)
    scaled = (
        values32
        * lax.rsqrt(jnp.mean(values32 * values32, axis=-1, keepdims=True) + epsilon)
        * gain_row
    )
    pair_count = scaled.shape[-1] // 4
    inv_freq = rotary_base ** (-jnp.arange(pair_count, dtype=jnp.float32) / pair_count)
    grid_row = (positions // GRID_W).astype(jnp.float32)
    grid_col = (positions % GRID_W).astype(jnp.float32)
    angles = jnp.concatenate([grid_row[:, None] * inv_freq, grid_col[:, None] * inv_freq], axis=-1)[
        :, None, :
    ]
    cosine = jnp.cos(angles)
    sine_part = jnp.sin(angles)
    first_half = scaled[..., 0::2]
    second_half = scaled[..., 1::2]
    turned = jnp.stack(
        [
            first_half * cosine - second_half * sine_part,
            first_half * sine_part + second_half * cosine,
        ],
        axis=-1,
    )
    return turned.reshape(scaled.shape).astype(jnp.bfloat16)


def span_length(row_count):
    length = min(row_count, 2048)
    while row_count % length:
        length -= 1
    return length


def rotated(query_rows, key_rows, value_rows, query_gain, key_gain):
    row_count = query_rows.shape[0]
    head_size = query_gain.shape[0]
    q_heads = query_rows.shape[1] // head_size
    kv_heads = key_rows.shape[1] // head_size
    positions = lax.axis_index("ep") * row_count + jnp.arange(row_count, dtype=jnp.int32)
    q_rot = rotate_heads(query_rows.reshape(row_count, q_heads, head_size), query_gain, positions)
    k_rot = rotate_heads(key_rows.reshape(row_count, kv_heads, head_size), key_gain, positions)
    key_value = jnp.stack([k_rot, value_rows.reshape(row_count, kv_heads, head_size)], axis=2)
    return q_rot, key_value.reshape(row_count, kv_heads * 2 * head_size)


def attend(q_rot, piece_rows):
    row_count, q_heads, head_size = q_rot.shape
    kv_heads = piece_rows.shape[1] // (2 * head_size)
    group = q_heads // kv_heads
    scale = head_size ** (-0.5)
    q_grouped = q_rot.reshape(row_count, kv_heads, group, head_size).transpose(1, 2, 0, 3)
    q_grouped = q_grouped.reshape(kv_heads, group * row_count, head_size)
    query_count = group * row_count
    initial = (
        jnp.full((kv_heads, query_count), -jnp.inf, jnp.float32),
        jnp.zeros((kv_heads, query_count), jnp.float32),
        jnp.zeros((kv_heads, query_count, head_size), jnp.float32),
    )

    def one_span(carried, span_rows):
        run_max, run_sum, mixed = carried
        keys_span = span_rows[:, :, 0, :]
        values_span = span_rows[:, :, 1, :]
        scores = (
            jnp.einsum("hrd,shd->hrs", q_grouped, keys_span, preferred_element_type=jnp.float32)
            * scale
        )
        new_max = jnp.maximum(run_max, jnp.max(scores, axis=-1))
        factor = jnp.exp(run_max - new_max)
        weights = jnp.exp(scores - new_max[..., None])
        run_sum = run_sum * factor + jnp.sum(weights, axis=-1)
        added = jnp.einsum(
            "hrs,shd->hrd",
            weights.astype(jnp.bfloat16),
            values_span,
            preferred_element_type=jnp.float32,
        )
        mixed = mixed * factor[..., None] + added
        return ((new_max, run_sum, mixed), None)

    piece_count = piece_rows.shape[0]
    length = span_length(piece_count)
    spans = piece_rows.reshape(piece_count // length, length, kv_heads, 2, head_size)
    carried, unused = lax.scan(one_span, initial, spans)
    run_max, run_sum, mixed = carried
    result = (mixed / run_sum[..., None]).astype(jnp.bfloat16)
    result = result.reshape(kv_heads, group, row_count, head_size).transpose(2, 0, 1, 3)
    return result.reshape(row_count, q_heads * head_size)


def slot_numbers(own_routes, experts, capacity):
    tok_rows = own_routes.shape[0]
    named = own_routes[:, :, None] == jnp.arange(experts, dtype=jnp.int32)
    counts = jnp.any(named, axis=1).astype(jnp.bfloat16)
    rows = jnp.arange(tok_rows, dtype=jnp.int32)
    before = (rows[:, None] > rows[None, :]).astype(jnp.bfloat16)
    earlier = jnp.dot(before, counts, preferred_element_type=jnp.float32)
    ranks = jnp.sum(jnp.where(named, earlier[:, None, :], 0.0), axis=2).astype(jnp.int32)
    return own_routes * capacity + ranks


def hidden_of(rows_in, w_gate, w_up):
    gate_proj = jnp.einsum("...rd,...df->...rf", rows_in, w_gate, preferred_element_type=jnp.float32)
    up_proj = jnp.einsum("...rd,...df->...rf", rows_in, w_up, preferred_element_type=jnp.float32)
    return lax.optimization_barrier((jax.nn.silu(gate_proj) * up_proj).astype(jnp.bfloat16))


def plain_body(
    query_rows,
    key_rows,
    value_rows,
    query_gain,
    key_gain,
    moe_tokens,
    norm_gain,
    routes,
    route_weights,
    expert_gate,
    expert_up,
    expert_down,
    shared_gate,
    shared_up,
    shared_down,
):
    tok_rows, model_width = moe_tokens.shape
    top_count = routes.shape[1]
    tp_size = lax.axis_size("tp")
    ep_size = lax.axis_size("ep")
    local_experts = expert_gate.shape[0]
    experts = local_experts * ep_size
    capacity = 2 * tok_rows * top_count // experts
    lane = lax.axis_index("tp")

    all_gate, _ = doubled([expert_gate], "tp")
    all_up, _ = doubled([expert_up], "tp")
    all_down, _ = doubled([expert_down], "tp")

    values32 = moe_tokens.astype(jnp.float32)
    normed = (
        values32
        * lax.rsqrt(jnp.mean(values32 * values32, axis=-1, keepdims=True) + epsilon)
        * norm_gain
    ).astype(jnp.bfloat16)
    own_routes = lax.dynamic_slice_in_dim(routes, lane * tok_rows, tok_rows, 0)
    own_weights = lax.dynamic_slice_in_dim(route_weights, lane * tok_rows, tok_rows, 0)
    own_gates = own_weights / jnp.sum(own_weights, axis=-1, keepdims=True) * routed_scale
    slots = slot_numbers(own_routes, experts, capacity)
    slot_ids = jnp.arange(experts * capacity, dtype=jnp.int32)
    placing = jnp.any(slot_ids[:, None, None] == slots[None, :, :], axis=2).astype(jnp.bfloat16)
    send = jnp.dot(placing, normed, preferred_element_type=jnp.float32).astype(jnp.bfloat16)
    send = send.reshape(ep_size, local_experts * capacity, model_width)

    q_rot, key_value = rotated(query_rows, key_rows, value_rows, query_gain, key_gain)

    group_rows, masks = doubled([normed], "tp")
    arrived, pieces = exchange((send, key_value), (("ep", True), ("ep", False)), 1)
    attn_out = attend(q_rot, pieces.reshape(-1, pieces.shape[-1]))
    group_rows = jnp.concatenate([group_rows[masks.index(i)] for i in range(tp_size)], axis=0)
    shared_hidden = hidden_of(group_rows, shared_gate, shared_up)
    shared_part = jnp.dot(shared_hidden, shared_down, preferred_element_type=jnp.float32)
    shared_part = shared_part.astype(jnp.bfloat16).reshape(tp_size, tok_rows, model_width)

    arrived = arrived.reshape(ep_size, local_experts, capacity, model_width).transpose(1, 0, 2, 3)
    arrived = arrived.reshape(local_experts, ep_size * capacity, model_width)
    total = 0.0
    for part in range(tp_size):
        hidden = hidden_of(arrived, all_gate[part], all_up[part])
        partial = jnp.einsum(
            "lrf,lfd->lrd", hidden, all_down[part], preferred_element_type=jnp.float32
        )
        total = total + partial.astype(jnp.bfloat16).astype(jnp.float32)
    outgoing = total.astype(jnp.bfloat16).reshape(local_experts, ep_size, capacity, model_width)
    outgoing = outgoing.transpose(1, 0, 2, 3).reshape(
        ep_size, local_experts * capacity, model_width
    )
    returned, shared_parts = exchange((outgoing, shared_part), (("ep", True), ("tp", True)), 2)

    flat_rows = returned.reshape(experts * capacity, model_width)
    moe_out = jnp.sum(shared_parts.astype(jnp.float32), axis=0)
    for k in range(top_count):
        choosing = (slots[:, k, None] == slot_ids[None, :]).astype(jnp.bfloat16)
        picked = jnp.dot(choosing, flat_rows, preferred_element_type=jnp.float32)
        moe_out = moe_out + own_gates[:, k, None] * picked
    return (attn_out, moe_out.astype(jnp.bfloat16))


PARTS = 4
CHUNKS = 4
INNER = 2
VMEM_LIMIT = 56 * 1024 * 1024


def fused_kernel(
    sizes,
    routes_hbm,
    weights_hbm,
    tokens_hbm,
    norm_hbm,
    q_hbm,
    k_hbm,
    v_hbm,
    q_gain_hbm,
    k_gain_hbm,
    freq_hbm,
    gate_hbm,
    up_hbm,
    down_hbm,
    sgate_hbm,
    sup_hbm,
    sdown_hbm,
    attn_ref,
    moe_ref,
    routes_ref,
    weights_ref,
    tokens_ref,
    norm_ref,
    q_ref,
    k_ref,
    v_ref,
    q_gain_ref,
    k_gain_ref,
    freq_ref,
    w_gate,
    w_up,
    w_down,
    s_gate,
    s_up,
    s_down,
    normed_ref,
    tables,
    send,
    arrived,
    slot_gates,
    picks,
    plane,
    sideways,
    flow_out,
    flow_in,
    hidden,
    gate_acc,
    s_hidden,
    pieces,
    q_rot,
    other_rows,
    part_out,
    part_in,
    total,
    small_sems,
    load_sems,
    core_sems,
    y_sems,
    relay_sems,
    slot_sems,
    table_sems,
    kv_sems,
    side_sems,
    flow_sems,
):
    n_ep, capacity, top = sizes
    steps = n_ep // INNER
    me, lane = lax.axis_index("ep"), lax.axis_index("tp")
    spot = lax.div(me, INNER)
    core, across, beside = {"tp": flip(lane, 1)}, {"tp": flip(lane, 2)}, {"ep": flip(me, 1)}
    rows, width = normed_ref.shape
    chunk = width // CHUNKS
    bf16, f32 = jnp.bfloat16, jnp.float32

    def remote(source, target, sems, i, device):
        return pltpu.make_async_remote_copy(
            src_ref=source,
            dst_ref=target,
            send_sem=sems.at[(0,) + i],
            recv_sem=sems.at[(1,) + i],
            device_id=device,
            device_id_type=MESH,
        )

    def columns(q):
        return pl.ds(q * chunk, chunk)

    own_rows = pl.ds(pl.multiple_of(lane * rows, rows), rows)
    small = [
        pltpu.make_async_copy(source, target, small_sems.at[j])
        for j, (source, target) in enumerate(
            [
                (tokens_hbm, tokens_ref),
                (norm_hbm, norm_ref),
                (routes_hbm.at[:, own_rows], routes_ref),
                (weights_hbm.at[:, own_rows], weights_ref),
                (q_hbm, q_ref),
                (k_hbm, k_ref),
                (v_hbm, v_ref),
                (q_gain_hbm, q_gain_ref),
                (k_gain_hbm, k_gain_ref),
                (freq_hbm, freq_ref),
            ]
        )
    ]
    own = [
        (gate_hbm.at[0], w_gate),
        (up_hbm.at[0], w_up),
        (down_hbm.at[0], w_down),
        (sgate_hbm, s_gate),
        (sup_hbm, s_up),
        (sdown_hbm, s_down),
    ]
    loads = [
        pltpu.make_async_copy(source, target.at[0], load_sems.at[j])
        for j, (source, target) in enumerate(own)
    ]
    to_core = [
        remote(source, target.at[1], core_sems, (j,), core)
        for j, (source, target) in enumerate(own)
    ]
    to_across = [
        remote(source, target, y_sems, (j,), across)
        for j, (source, target) in enumerate(
            [(gate_hbm.at[0], w_gate.at[2]), (up_hbm.at[0], w_up.at[2])]
            + [
                (down_hbm.at[0, :, columns(q)], w_down.at[2, :, columns(q)])
                for q in range(CHUNKS)
            ]
            + [(normed_ref, other_rows), (part_out, part_in)]
        )
    ]
    rows_across, parts_across = to_across[2 + CHUNKS], to_across[3 + CHUNKS]
    relayed = [
        remote(source, target, relay_sems, (j,), core)
        for j, (source, target) in enumerate(
            [(w_gate.at[2], w_gate.at[3]), (w_up.at[2], w_up.at[3])]
            + [(w_down.at[2, :, columns(q)], w_down.at[3, :, columns(q)]) for q in range(CHUNKS)]
        )
    ]

    def slots_to(i):
        return remote(send.at[i], arrived.at[i], slot_sems, (i,), {"ep": flip(me, i)})

    def table_to(i):
        return remote(tables.at[0], tables.at[i], table_sems, (i,), {"ep": flip(me, i)})

    def pieces_to(i):
        return remote(pieces.at[me], pieces.at[me], kv_sems, (i,), {"ep": flip(me, i)})

    def side_to(q, j):
        target = plane.at[j, pl.ds(capacity, capacity), columns(q)]
        return remote(sideways.at[j, :, columns(q)], target, side_sems, (q, j), beside)

    def flow_to(q, way, index):
        ahead = {"ep": lax.rem(me + (INNER if way == 0 else n_ep - INNER), n_ep)}
        return remote(
            flow_out.at[way, index, :, columns(q)],
            flow_in.at[way, index, :, columns(q)],
            flow_sems,
            (way, index, q),
            ahead,
        )

    def chosen_by(i, expert):
        base = (expert * capacity).astype(f32)
        index = lax.broadcasted_iota(jnp.int32, (capacity, rows), 0).astype(f32) + base
        return [index == tables[i, k : k + 1, :] for k in range(top)]

    def one_hot(i, expert):
        chosen = chosen_by(i, expert)
        return jnp.where(functools.reduce(jnp.logical_or, chosen), 1.0, 0.0).astype(bf16)

    def place(i):
        chosen = one_hot(0, flip(me, i))
        packed = jnp.dot(chosen, normed_ref[...], preferred_element_type=f32).astype(bf16)
        if i:
            send[i] = packed
        else:
            arrived[0] = packed

    barrier = pltpu.get_barrier_semaphore()
    for device in [core, across] + [{"ep": flip(me, i)} for i in range(1, n_ep)]:
        pl.semaphore_signal(barrier, inc=1, device_id=device, device_id_type=MESH)
    for load in small + loads:
        load.start()
    pl.semaphore_wait(barrier, n_ep + 1)
    for copy in to_across[:2] + to_core:
        copy.start()

    for load in small:
        load.wait()
    experts = lax.broadcasted_iota(jnp.int32, (n_ep, rows), 0)
    named = [experts == routes_ref[k : k + 1, :] for k in range(top)]
    counted = jnp.where(functools.reduce(jnp.logical_or, named), 1.0, 0.0).astype(bf16)
    at0 = lax.broadcasted_iota(jnp.int32, (rows, rows), 0)
    at1 = lax.broadcasted_iota(jnp.int32, (rows, rows), 1)
    before = jnp.where(at0 < at1, 1.0, 0.0).astype(bf16)
    earlier = jnp.dot(counted, before, preferred_element_type=f32)
    weight_sum = jnp.sum(weights_ref[...], axis=0, keepdims=True)
    for k in range(top):
        rank = jnp.sum(jnp.where(named[k], earlier, 0.0), axis=0, keepdims=True)
        tables[0, k : k + 1, :] = (routes_ref[k : k + 1, :] * capacity).astype(f32) + rank
        tables[0, top + k : top + k + 1, :] = weights_ref[k : k + 1, :] / weight_sum * routed_scale
    for r in range(0, rows, 16):
        values = tokens_ref[r : r + 16, :].astype(f32)
        mean = jnp.mean(values * values, axis=-1, keepdims=True)
        normed_ref[r : r + 16, :] = (values * lax.rsqrt(mean + epsilon) * norm_ref[...]).astype(bf16)
    place(1)
    for i in range(1, n_ep):
        table_to(i).start()
    for i in range(1, n_ep):
        if i + 1 < n_ep:
            place(i + 1)
        slots_to(i).start()
    place(0)

    head = q_gain_ref.shape[1]
    q_heads = q_ref.shape[1] // head
    row_count = q_ref.shape[0]
    position = lax.broadcasted_iota(jnp.int32, (row_count, 2 * head), 0) + me * row_count
    in_lane = lax.broadcasted_iota(jnp.int32, (row_count, 2 * head), 1)
    by_row = lax.rem(in_lane, head) < head // 2
    angle = jnp.where(by_row, lax.div(position, GRID_W), lax.rem(position, GRID_W)).astype(f32)
    angle = angle * freq_ref[...]
    even = lax.rem(in_lane, 2) == 0
    cosine = jnp.cos(angle)
    sine = jnp.where(even, -jnp.sin(angle), jnp.sin(angle))

    def turned(scaled):
        span = scaled.shape[1]
        swapped = jnp.where(even, pltpu.roll(scaled, span - 1, 1), pltpu.roll(scaled, 1, 1))
        return scaled * cosine + swapped * sine

    def factor_of(values):
        return lax.rsqrt(jnp.mean(values * values, axis=-1, keepdims=True) + epsilon)

    key_value = jnp.concatenate([k_ref[...].astype(f32), v_ref[...].astype(f32)], axis=0).T
    key32 = key_value[:, :head]
    key32 = key32 * factor_of(key32) * k_gain_ref[...]
    spun = turned(jnp.concatenate([key32, key_value[:, head:]], axis=1))
    pieces[me] = jnp.where(in_lane < head, spun, key_value).astype(bf16)
    scale = head ** (-0.5)
    for h in range(0, q_heads, 2):
        pair = [q_ref[:, (h + j) * head : (h + j + 1) * head].astype(f32) for j in range(2)]
        pair = [x * factor_of(x) * q_gain_ref[...] for x in pair]
        spun = turned(jnp.concatenate(pair, axis=1)).astype(bf16) * jnp.asarray(scale, bf16)
        zero = jnp.zeros((row_count, head), bf16)
        for j in range(2):
            q_rot[h + j] = jnp.concatenate([spun[:, j * head : (j + 1) * head], zero], axis=1)
    for i in range(1, n_ep):
        pieces_to(i).start()

    for i in range(1, n_ep):
        table_to(i).wait()
    for i in range(n_ep):
        chosen = chosen_by(i, me)
        found = 0.0
        for k in range(top):
            found = found + jnp.where(chosen[k], tables[i, top + k : top + k + 1, :], 0.0)
        slot_gates[i * capacity : (i + 1) * capacity, :] = jnp.sum(found, axis=1, keepdims=True)
    for j in range(steps):
        picks[j, :capacity, :] = one_hot(INNER * j, me)
        picks[j, capacity:, :] = one_hot(INNER * j, flip(me, 1))

    half = n_ep // 2
    group_rows = half * capacity

    def rows_of(g):
        return arrived[g * half : (g + 1) * half].reshape(group_rows, width)

    def span_of(g):
        return pl.ds(g * group_rows, group_rows)

    def gate_of(p, g):
        gate_acc[p, span_of(g), :] = jnp.dot(rows_of(g), w_gate[p], preferred_element_type=f32)

    def hidden_at(p, g):
        up_proj = jnp.dot(rows_of(g), w_up[p], preferred_element_type=f32)
        gate_proj = gate_acc[p, span_of(g), :]
        hidden[p, span_of(g), :] = (jax.nn.silu(gate_proj) * up_proj).astype(bf16)

    for i in range(1, half):
        slots_to(i).wait_recv()
    for load in loads:
        load.wait()
    gate_of(0, 0)
    hidden_at(0, 0)
    for copy in to_core:
        copy.wait()
    gate_of(1, 0)
    hidden_at(1, 0)
    to_across[0].wait()
    relayed[0].start()
    for copy in to_across[2:4] + [rows_across] + to_across[4 : 2 + CHUNKS]:
        copy.start()
    gate_of(2, 0)
    relayed[0].wait()
    gate_of(3, 0)
    for i in range(half, n_ep):
        slots_to(i).wait_recv()
    gate_of(0, 1)
    hidden_at(0, 1)
    gate_of(1, 1)
    hidden_at(1, 1)
    gate_of(2, 1)
    gate_of(3, 1)
    to_across[1].wait()
    relayed[1].start()
    for g in range(2):
        hidden_at(2, g)
    relayed[1].wait()
    for g in range(2):
        hidden_at(3, g)

    def down(q):
        to_across[2 + q].wait()
        relayed[2 + q].start()
        relayed[2 + q].wait()
        for g in reversed(range(2)):
            summed = 0.0
            for p in range(PARTS):
                partial = jnp.dot(
                    hidden[p, span_of(g), :], w_down[p, :, columns(q)], preferred_element_type=f32
                )
                summed = summed + partial.astype(bf16).astype(f32)
            summed = summed.astype(bf16).astype(f32) * slot_gates[span_of(g), :]
            summed = summed.astype(bf16)
            for j in range(half):
                i = g * half + j
                block = summed[j * capacity : (j + 1) * capacity]
                if i % INNER:
                    sideways[i // INNER, :, columns(q)] = block
                else:
                    plane[i // INNER, :capacity, columns(q)] = block
        for j in reversed(range(steps)):
            side_to(q, j).start()

    def contribution(j, q):
        return lax.dot_general(
            picks[j], plane[j, :, columns(q)], (((0,), (0,)), ((), ())), preferred_element_type=f32
        )

    def crossed(a, b):
        result, bit = 0, 1
        while bit < steps:
            differs = lax.rem(lax.rem(lax.div(a, bit), 2) + lax.rem(lax.div(b, bit), 2), 2)
            result, bit = result + bit * differs, 2 * bit
        return result

    def inside(place_at):
        return (place_at >= 0) & (place_at < steps)

    def emit(q, distance, fed):
        for way in range(2):
            sign = 1 - 2 * way
            target = spot + sign * distance
            behind = inside(spot - sign)

            @pl.when(inside(target) & (behind if fed else jnp.logical_not(behind)))
            def _(way=way, target=target):
                summed = contribution(crossed(spot, target), q)
                if fed:
                    flow_to(q, way, distance).wait_recv()
                    summed = summed + flow_in[way, distance, :, columns(q)].astype(f32)
                flow_out[way, distance - 1, :, columns(q)] = summed.astype(bf16)
                flow_to(q, way, distance - 1).start()

    def edges(q):
        for j in range(steps):
            side_to(q, j).wait()
        for distance in reversed(range(1, steps)):
            emit(q, distance, False)

    def keep(q):
        total[:, columns(q)] += contribution(0, q)
        for way in range(2):

            @pl.when(inside(spot - (1 - 2 * way)))
            def _(way=way):
                flow_to(q, way, 0).wait_recv()
                total[:, columns(q)] += flow_in[way, 0, :, columns(q)].astype(f32)

    def shared_hidden(source, p):
        gate_proj = jnp.dot(source[...], s_gate[p], preferred_element_type=f32)
        up_proj = jnp.dot(source[...], s_up[p], preferred_element_type=f32)
        s_hidden[p] = (jax.nn.silu(gate_proj) * up_proj).astype(bf16)

    def shared_down(q):
        summed = 0.0
        for p in range(2):
            partial = jnp.dot(s_hidden[p], s_down[p, :, columns(q)], preferred_element_type=f32)
            summed = summed + partial.astype(bf16).astype(f32)
        return summed

    def shared_own():
        for p in range(2):
            shared_hidden(normed_ref, p)
        for q in range(CHUNKS):
            total[:, columns(q)] = shared_down(q)

    def shared_other():
        rows_across.wait()
        for p in range(2):
            shared_hidden(other_rows, p)
        for q in range(CHUNKS):
            part_out[:, columns(q)] = shared_down(q).astype(bf16)
        parts_across.start()

    block = math.gcd(row_count, 128)

    def attend_head(h):
        def one_block(b, c):
            at = pl.ds(pl.multiple_of(b * block, block), block)
            keys = pieces[...].reshape(n_ep * row_count, 2 * head)
            scores = lax.dot_general(
                q_rot[h, at, :], keys, (((1,), (1,)), ((), ())), preferred_element_type=f32
            )
            weights = jnp.exp(scores - jnp.max(scores, axis=-1, keepdims=True))
            row_sum = jnp.sum(weights, axis=-1, keepdims=True)
            mixed = jnp.dot(weights.astype(bf16), keys, preferred_element_type=f32)
            attn_ref[at, h * head : (h + 1) * head] = (mixed / row_sum)[:, head:].astype(bf16)
            return c

        lax.fori_loop(0, row_count // block, one_block, 0)

    for step in range(CHUNKS + steps):
        if step == 2:
            shared_other()
        if step < CHUNKS:
            down(step)
        if step == 0:
            shared_own()
        for hop in range(steps + 1):
            q = step - 1 - hop
            if 0 <= q < CHUNKS:
                if hop == 0:
                    edges(q)
                elif hop < steps - 1:
                    emit(q, steps - 1 - hop, True)
                elif hop == steps - 1:
                    keep(q)
        if step == 1:
            for i in range(1, n_ep):
                pieces_to(i).wait()
        if 1 <= step < CHUNKS + 1:
            for h in range((step - 1) * q_heads // CHUNKS, step * q_heads // CHUNKS):
                attend_head(h)

    parts_across.wait()
    for q in range(CHUNKS):
        part = part_in[:, columns(q)].astype(f32)
        moe_ref[:, columns(q)] = (total[:, columns(q)] + part).astype(bf16)
    for i in range(1, n_ep):
        slots_to(i).wait_send()
    for way in range(2):
        for distance in range(1, steps):

            @pl.when(inside(spot + (1 - 2 * way) * distance))
            def _(way=way, distance=distance):
                for q in range(CHUNKS):
                    flow_to(q, way, distance - 1).wait_send()


def fused_body(
    query_rows,
    key_rows,
    value_rows,
    query_gain,
    key_gain,
    moe_tokens,
    norm_gain,
    routes,
    route_weights,
    expert_gate,
    expert_up,
    expert_down,
    shared_gate,
    shared_up,
    shared_down,
):
    tok_rows, model_width = moe_tokens.shape
    row_count = query_rows.shape[0]
    head_size = query_gain.shape[0]
    top_count = routes.shape[1]
    ep_size = lax.axis_size("ep")
    capacity = 2 * tok_rows * top_count // ep_size
    units = expert_gate.shape[2]
    steps = ep_size // INNER
    pair_count = head_size // 4
    pair = (np.arange(2 * head_size) % head_size) // 2 % pair_count
    inv_freq = rotary_base ** (-jnp.asarray(pair, jnp.float32) / pair_count)

    bf16, f32 = jnp.bfloat16, jnp.float32
    vmem, anywhere = pl.BlockSpec(memory_space=pltpu.VMEM), pl.BlockSpec(memory_space=pl.ANY)
    dma = pltpu.SemaphoreType.DMA
    all_rows = ep_size * capacity
    token_shape = (tok_rows, model_width)
    small = [
        routes.T,
        route_weights.T,
        moe_tokens,
        norm_gain[None],
        query_rows,
        key_rows.T,
        value_rows.T,
        query_gain[None],
        key_gain[None],
        inv_freq[None],
    ]
    held = [x.shape for x in small]
    held[0] = held[1] = (top_count, tok_rows)
    return pl.pallas_call(
        functools.partial(fused_kernel, (ep_size, capacity, top_count)),
        out_shape=[
            jax.ShapeDtypeStruct(query_rows.shape, bf16),
            jax.ShapeDtypeStruct(moe_tokens.shape, bf16),
        ],
        in_specs=[anywhere] * 16,
        out_specs=[vmem] * 2,
        scratch_shapes=[pltpu.VMEM(shape, x.dtype) for shape, x in zip(held, small)]
        + [
            pltpu.VMEM((PARTS, model_width, units), bf16),
            pltpu.VMEM((PARTS, model_width, units), bf16),
            pltpu.VMEM((PARTS, units, model_width), bf16),
            pltpu.VMEM((2, model_width, units), bf16),
            pltpu.VMEM((2, model_width, units), bf16),
            pltpu.VMEM((2, units, model_width), bf16),
            pltpu.VMEM(token_shape, bf16),
            pltpu.VMEM((ep_size, 8, tok_rows), f32),
            pltpu.VMEM((ep_size, capacity, model_width), bf16),
            pltpu.VMEM((ep_size, capacity, model_width), bf16),
            pltpu.VMEM((all_rows, 1), f32),
            pltpu.VMEM((steps, 2 * capacity, tok_rows), bf16),
            pltpu.VMEM((steps, 2 * capacity, model_width), bf16),
            pltpu.VMEM((steps, capacity, model_width), bf16),
            pltpu.VMEM((2, steps - 1) + token_shape, bf16),
            pltpu.VMEM((2, steps - 1) + token_shape, bf16),
            pltpu.VMEM((PARTS, all_rows, units), bf16),
            pltpu.VMEM((PARTS, all_rows, units), f32),
            pltpu.VMEM((2, tok_rows, units), bf16),
            pltpu.VMEM((ep_size, row_count, 2 * head_size), bf16),
            pltpu.VMEM((query_rows.shape[1] // head_size, row_count, 2 * head_size), bf16),
            pltpu.VMEM(token_shape, bf16),
            pltpu.VMEM(token_shape, bf16),
            pltpu.VMEM(token_shape, bf16),
            pltpu.VMEM(token_shape, f32),
            dma((10,)),
            dma((6,)),
            dma((2, 6)),
            dma((2, 4 + CHUNKS)),
            dma((2, 2 + CHUNKS)),
            dma((2, ep_size)),
            dma((2, ep_size)),
            dma((2, ep_size)),
            dma((2, CHUNKS, steps)),
            dma((2, 2, steps - 1, CHUNKS)),
        ],
        compiler_params=pltpu.CompilerParams(
            collective_id=3, has_side_effects=True, vmem_limit_bytes=VMEM_LIMIT
        ),
    )(
        *small,
        expert_gate,
        expert_up,
        expert_down,
        shared_gate,
        shared_up,
        shared_down,
    )


def body(*arrays):
    query_rows, query_gain, moe_tokens, routes = arrays[0], arrays[3], arrays[5], arrays[7]
    expert_gate = arrays[9]
    ep_size, tp_size = lax.axis_size("ep"), lax.axis_size("tp")
    capacity = 2 * moe_tokens.shape[0] * routes.shape[1] // (ep_size * expert_gate.shape[0])
    head_size = query_gain.shape[0]
    one_kernel = (
        tp_size == PARTS
        and expert_gate.shape[0] == 1
        and ep_size & (ep_size - 1) == 0
        and capacity % 16 == 0
        and ep_size >= 2 * INNER
        and 2 * routes.shape[1] <= 8
        and moe_tokens.shape[0] % 128 == 0
        and ep_size * query_rows.shape[0] * 2 * head_size <= 1 << 20
        and query_rows.shape[1] // head_size % 2 == 0
        and arrays[1].shape[1] == head_size
        and 2 * head_size % 128 == 0
        and math.log2(head_size) % 2 == 0
    )
    return fused_body(*arrays) if one_kernel else plain_body(*arrays)


def solution(mesh):
    return jax.shard_map(
        body,
        mesh=mesh,
        in_specs=(
            P("ep", "tp"),
            P("ep", "tp"),
            P("ep", "tp"),
            P(),
            P(),
            P(("ep", "tp"), None),
            P(),
            P("ep", None),
            P("ep", None),
            P("ep", None, "tp"),
            P("ep", None, "tp"),
            P("ep", "tp", None),
            P(None, "tp"),
            P(None, "tp"),
            P("tp", None),
        ),
        out_specs=(P("ep", "tp"), P(("ep", "tp"), None)),
        check_vma=False,
    )
```

```python
import functools
import math

import jax
import jax.numpy as jnp
import numpy as np
from jax import lax
from jax.experimental import pallas as pl
from jax.experimental.pallas import tpu as pltpu
from jax.sharding import PartitionSpec as P

GRID_W = 64
MESH = pl.DeviceIdType.MESH


epsilon = 1e-06
rotary_base = 10000.0
routed_scale = 2.5


def flip(number, mask):
    result, bit = number, 1
    while bit <= mask:
        if mask & bit:
            result = result + bit - 2 * bit * lax.rem(lax.div(number, bit), 2)
        bit *= 2
    return result


def doubled(blocks, axis):
    n = lax.axis_size(axis)
    masks, step = [0], n // 2
    while step:
        pairs = [(j, j ^ step) for j in range(n)]
        blocks = blocks + [lax.ppermute(block, axis, pairs) for block in blocks]
        masks = masks + [mask ^ step for mask in masks]
        step //= 2
    return blocks, masks


def each_peer(axis, sizes, step):
    if axis == "tp":
        for i in range(1, sizes[axis]):
            step(i, 0)
    else:
        lax.fori_loop(1, sizes[axis], step, 0)


def exchange_kernel(plan, sizes, *refs):
    count = len(plan)
    sources, targets = refs[:count], refs[count : 2 * count]
    send_sems = refs[2 * count : 3 * count]
    recv_sems = refs[3 * count : 4 * count]
    own_sems = refs[4 * count]
    axes = []
    for axis, _ in plan:
        if axis not in axes:
            axes.append(axis)
    barrier = pltpu.get_barrier_semaphore()
    for axis in axes:
        me, n = lax.axis_index(axis), sizes[axis]

        def greet(i, c, axis=axis, me=me, n=n):
            pl.semaphore_signal(
                barrier, inc=1, device_id={axis: lax.rem(me + i, n)}, device_id_type=MESH
            )
            return c

        lax.fori_loop(1, n, greet, 0)
    pl.semaphore_wait(barrier, sum(sizes[axis] - 1 for axis in axes))

    def copy_of(k, i):
        axis, scattered = plan[k]
        me, n = lax.axis_index(axis), sizes[axis]
        if axis == "tp":
            peer, source_at, target_at = flip(me, i), i, i
        else:
            peer = lax.rem(me + i, n)
            source_at, target_at = peer, me
        return pltpu.make_async_remote_copy(
            src_ref=sources[k].at[source_at] if scattered else sources[k],
            dst_ref=targets[k].at[target_at],
            send_sem=send_sems[k].at[i],
            recv_sem=recv_sems[k].at[i],
            device_id={axis: peer},
            device_id_type=MESH,
        )

    for k, (axis, scattered) in enumerate(plan):

        def begin(i, c, k=k):
            copy_of(k, i).start()
            return c

        each_peer(axis, sizes, begin)
    local = []
    for k, (axis, scattered) in enumerate(plan):
        me = 0 if axis == "tp" else lax.axis_index(axis)
        copy = pltpu.make_async_copy(
            sources[k].at[me] if scattered else sources[k], targets[k].at[me], own_sems.at[k]
        )
        copy.start()
        local.append(copy)
    for copy in local:
        copy.wait()
    for k, (axis, scattered) in enumerate(plan):

        def finish(i, c, k=k):
            copy_of(k, i).wait()
            return c

        each_peer(axis, sizes, finish)


def exchange(operands, plan, number):
    sizes = {axis: lax.axis_size(axis) for axis, _ in plan}
    shapes = []
    for array, (axis, scattered) in zip(operands, plan):
        shape = array.shape if scattered else (sizes[axis],) + array.shape
        shapes.append(jax.ShapeDtypeStruct(shape, array.dtype))
    sems = [pltpu.SemaphoreType.DMA((sizes[axis],)) for axis, _ in plan]
    traffic = 2 * sum(s.size * s.dtype.itemsize for s in shapes)
    return pl.pallas_call(
        functools.partial(exchange_kernel, plan, sizes),
        out_shape=shapes,
        in_specs=[pl.BlockSpec(memory_space=pl.ANY)] * len(plan),
        out_specs=[pl.BlockSpec(memory_space=pl.ANY)] * len(plan),
        scratch_shapes=sems + sems + [pltpu.SemaphoreType.DMA((len(plan),))],
        compiler_params=pltpu.CompilerParams(collective_id=number, has_side_effects=True),
        cost_estimate=pl.CostEstimate(
            flops=0, bytes_accessed=16 * traffic, transcendentals=0
        ),
    )(*operands)


def rotate_heads(heads_in, gain_row, positions):
    values32 = heads_in.astype(jnp.float32)
    scaled = (
        values32
        * lax.rsqrt(jnp.mean(values32 * values32, axis=-1, keepdims=True) + epsilon)
        * gain_row
    )
    pair_count = scaled.shape[-1] // 4
    inv_freq = rotary_base ** (-jnp.arange(pair_count, dtype=jnp.float32) / pair_count)
    grid_row = (positions // GRID_W).astype(jnp.float32)
    grid_col = (positions % GRID_W).astype(jnp.float32)
    angles = jnp.concatenate([grid_row[:, None] * inv_freq, grid_col[:, None] * inv_freq], axis=-1)[
        :, None, :
    ]
    cosine = jnp.cos(angles)
    sine_part = jnp.sin(angles)
    first_half = scaled[..., 0::2]
    second_half = scaled[..., 1::2]
    turned = jnp.stack(
        [
            first_half * cosine - second_half * sine_part,
            first_half * sine_part + second_half * cosine,
        ],
        axis=-1,
    )
    return turned.reshape(scaled.shape).astype(jnp.bfloat16)


def span_length(row_count):
    length = min(row_count, 2048)
    while row_count % length:
        length -= 1
    return length


def rotated(query_rows, key_rows, value_rows, query_gain, key_gain):
    row_count = query_rows.shape[0]
    head_size = query_gain.shape[0]
    q_heads = query_rows.shape[1] // head_size
    kv_heads = key_rows.shape[1] // head_size
    positions = lax.axis_index("ep") * row_count + jnp.arange(row_count, dtype=jnp.int32)
    q_rot = rotate_heads(query_rows.reshape(row_count, q_heads, head_size), query_gain, positions)
    k_rot = rotate_heads(key_rows.reshape(row_count, kv_heads, head_size), key_gain, positions)
    key_value = jnp.stack([k_rot, value_rows.reshape(row_count, kv_heads, head_size)], axis=2)
    return q_rot, key_value.reshape(row_count, kv_heads * 2 * head_size)


def attend(q_rot, piece_rows):
    row_count, q_heads, head_size = q_rot.shape
    kv_heads = piece_rows.shape[1] // (2 * head_size)
    group = q_heads // kv_heads
    scale = head_size ** (-0.5)
    q_grouped = q_rot.reshape(row_count, kv_heads, group, head_size).transpose(1, 2, 0, 3)
    q_grouped = q_grouped.reshape(kv_heads, group * row_count, head_size)
    query_count = group * row_count
    initial = (
        jnp.full((kv_heads, query_count), -jnp.inf, jnp.float32),
        jnp.zeros((kv_heads, query_count), jnp.float32),
        jnp.zeros((kv_heads, query_count, head_size), jnp.float32),
    )

    def one_span(carried, span_rows):
        run_max, run_sum, mixed = carried
        keys_span = span_rows[:, :, 0, :]
        values_span = span_rows[:, :, 1, :]
        scores = (
            jnp.einsum("hrd,shd->hrs", q_grouped, keys_span, preferred_element_type=jnp.float32)
            * scale
        )
        new_max = jnp.maximum(run_max, jnp.max(scores, axis=-1))
        factor = jnp.exp(run_max - new_max)
        weights = jnp.exp(scores - new_max[..., None])
        run_sum = run_sum * factor + jnp.sum(weights, axis=-1)
        added = jnp.einsum(
            "hrs,shd->hrd",
            weights.astype(jnp.bfloat16),
            values_span,
            preferred_element_type=jnp.float32,
        )
        mixed = mixed * factor[..., None] + added
        return ((new_max, run_sum, mixed), None)

    piece_count = piece_rows.shape[0]
    length = span_length(piece_count)
    spans = piece_rows.reshape(piece_count // length, length, kv_heads, 2, head_size)
    carried, unused = lax.scan(one_span, initial, spans)
    run_max, run_sum, mixed = carried
    result = (mixed / run_sum[..., None]).astype(jnp.bfloat16)
    result = result.reshape(kv_heads, group, row_count, head_size).transpose(2, 0, 1, 3)
    return result.reshape(row_count, q_heads * head_size)


def slot_numbers(own_routes, experts, capacity):
    tok_rows = own_routes.shape[0]
    named = own_routes[:, :, None] == jnp.arange(experts, dtype=jnp.int32)
    counts = jnp.any(named, axis=1).astype(jnp.bfloat16)
    rows = jnp.arange(tok_rows, dtype=jnp.int32)
    before = (rows[:, None] > rows[None, :]).astype(jnp.bfloat16)
    earlier = jnp.dot(before, counts, preferred_element_type=jnp.float32)
    ranks = jnp.sum(jnp.where(named, earlier[:, None, :], 0.0), axis=2).astype(jnp.int32)
    return own_routes * capacity + ranks


def hidden_of(rows_in, w_gate, w_up):
    gate_proj = jnp.einsum("...rd,...df->...rf", rows_in, w_gate, preferred_element_type=jnp.float32)
    up_proj = jnp.einsum("...rd,...df->...rf", rows_in, w_up, preferred_element_type=jnp.float32)
    return lax.optimization_barrier((jax.nn.silu(gate_proj) * up_proj).astype(jnp.bfloat16))


def plain_body(
    query_rows,
    key_rows,
    value_rows,
    query_gain,
    key_gain,
    moe_tokens,
    norm_gain,
    routes,
    route_weights,
    expert_gate,
    expert_up,
    expert_down,
    shared_gate,
    shared_up,
    shared_down,
):
    tok_rows, model_width = moe_tokens.shape
    top_count = routes.shape[1]
    tp_size = lax.axis_size("tp")
    ep_size = lax.axis_size("ep")
    local_experts = expert_gate.shape[0]
    experts = local_experts * ep_size
    capacity = 2 * tok_rows * top_count // experts
    lane = lax.axis_index("tp")

    all_gate, _ = doubled([expert_gate], "tp")
    all_up, _ = doubled([expert_up], "tp")
    all_down, _ = doubled([expert_down], "tp")

    values32 = moe_tokens.astype(jnp.float32)
    normed = (
        values32
        * lax.rsqrt(jnp.mean(values32 * values32, axis=-1, keepdims=True) + epsilon)
        * norm_gain
    ).astype(jnp.bfloat16)
    own_routes = lax.dynamic_slice_in_dim(routes, lane * tok_rows, tok_rows, 0)
    own_weights = lax.dynamic_slice_in_dim(route_weights, lane * tok_rows, tok_rows, 0)
    own_gates = own_weights / jnp.sum(own_weights, axis=-1, keepdims=True) * routed_scale
    slots = slot_numbers(own_routes, experts, capacity)
    slot_ids = jnp.arange(experts * capacity, dtype=jnp.int32)
    placing = jnp.any(slot_ids[:, None, None] == slots[None, :, :], axis=2).astype(jnp.bfloat16)
    send = jnp.dot(placing, normed, preferred_element_type=jnp.float32).astype(jnp.bfloat16)
    send = send.reshape(ep_size, local_experts * capacity, model_width)

    q_rot, key_value = rotated(query_rows, key_rows, value_rows, query_gain, key_gain)

    group_rows, masks = doubled([normed], "tp")
    arrived, pieces = exchange((send, key_value), (("ep", True), ("ep", False)), 1)
    attn_out = attend(q_rot, pieces.reshape(-1, pieces.shape[-1]))
    group_rows = jnp.concatenate([group_rows[masks.index(i)] for i in range(tp_size)], axis=0)
    shared_hidden = hidden_of(group_rows, shared_gate, shared_up)
    shared_part = jnp.dot(shared_hidden, shared_down, preferred_element_type=jnp.float32)
    shared_part = shared_part.astype(jnp.bfloat16).reshape(tp_size, tok_rows, model_width)

    arrived = arrived.reshape(ep_size, local_experts, capacity, model_width).transpose(1, 0, 2, 3)
    arrived = arrived.reshape(local_experts, ep_size * capacity, model_width)
    total = 0.0
    for part in range(tp_size):
        hidden = hidden_of(arrived, all_gate[part], all_up[part])
        partial = jnp.einsum(
            "lrf,lfd->lrd", hidden, all_down[part], preferred_element_type=jnp.float32
        )
        total = total + partial.astype(jnp.bfloat16).astype(jnp.float32)
    outgoing = total.astype(jnp.bfloat16).reshape(local_experts, ep_size, capacity, model_width)
    outgoing = outgoing.transpose(1, 0, 2, 3).reshape(
        ep_size, local_experts * capacity, model_width
    )
    returned, shared_parts = exchange((outgoing, shared_part), (("ep", True), ("tp", True)), 2)

    flat_rows = returned.reshape(experts * capacity, model_width)
    moe_out = jnp.sum(shared_parts.astype(jnp.float32), axis=0)
    for k in range(top_count):
        choosing = (slots[:, k, None] == slot_ids[None, :]).astype(jnp.bfloat16)
        picked = jnp.dot(choosing, flat_rows, preferred_element_type=jnp.float32)
        moe_out = moe_out + own_gates[:, k, None] * picked
    return (attn_out, moe_out.astype(jnp.bfloat16))


PARTS = 4
CHUNKS = 8
UP_PIECES = 2
PORTIONS = 2
INNER = 2
VMEM_LIMIT = 56 * 1024 * 1024


def fused_kernel(
    sizes,
    routes_hbm,
    weights_hbm,
    tokens_hbm,
    norm_hbm,
    q_hbm,
    k_hbm,
    v_hbm,
    q_gain_hbm,
    k_gain_hbm,
    freq_hbm,
    gate_hbm,
    up_hbm,
    down_hbm,
    sgate_hbm,
    sup_hbm,
    sdown_hbm,
    attn_ref,
    moe_ref,
    routes_ref,
    weights_ref,
    tokens_ref,
    norm_ref,
    q_ref,
    k_ref,
    v_ref,
    q_gain_ref,
    k_gain_ref,
    freq_ref,
    w_gate,
    w_up,
    w_down,
    s_gate,
    s_up,
    s_down,
    normed_ref,
    tables,
    blocks,
    send,
    arrived,
    slot_gates,
    picks,
    plane,
    sideways,
    flow_out,
    flow_in,
    hidden,
    gate_acc,
    s_hidden,
    pieces,
    q_rot,
    other_rows,
    part_out,
    part_in,
    total,
    small_sems,
    load_sems,
    core_sems,
    y_sems,
    relay_sems,
    block_sems,
    slot_sems,
    table_sems,
    kv_sems,
    kv_side_sems,
    side_sems,
    flow_sems,
):
    n_ep, capacity, top = sizes
    steps = n_ep // INNER
    me, lane = lax.axis_index("ep"), lax.axis_index("tp")
    spot = lax.div(me, INNER)
    core, across, beside = {"tp": flip(lane, 1)}, {"tp": flip(lane, 2)}, {"ep": flip(me, 1)}
    rows, width = normed_ref.shape
    chunk = width // CHUNKS
    bf16, f32 = jnp.bfloat16, jnp.float32

    def remote(source, target, sems, i, device):
        return pltpu.make_async_remote_copy(
            src_ref=source,
            dst_ref=target,
            send_sem=sems.at[(0,) + i],
            recv_sem=sems.at[(1,) + i],
            device_id=device,
            device_id_type=MESH,
        )

    def columns(q):
        return pl.ds(q * chunk, chunk)

    def portion(j):
        return pl.ds(j * (rows // PORTIONS), rows // PORTIONS)

    def piece(j):
        return pl.ds(j * (width // UP_PIECES), width // UP_PIECES)

    own_rows = pl.ds(pl.multiple_of(lane * rows, rows), rows)
    small = [
        pltpu.make_async_copy(source, target, small_sems.at[j])
        for j, (source, target) in enumerate(
            [
                (tokens_hbm, tokens_ref),
                (norm_hbm, norm_ref),
                (routes_hbm.at[:, own_rows], routes_ref),
                (weights_hbm.at[:, own_rows], weights_ref),
                (q_hbm, q_ref),
                (k_hbm, k_ref),
                (v_hbm, v_ref),
                (q_gain_hbm, q_gain_ref),
                (k_gain_hbm, k_gain_ref),
                (freq_hbm, freq_ref),
            ]
        )
    ]
    own = [
        (gate_hbm.at[0], w_gate),
        (up_hbm.at[0], w_up),
        (down_hbm.at[0], w_down),
        (sgate_hbm, s_gate),
        (sup_hbm, s_up),
        (sdown_hbm, s_down),
    ]
    loads = [
        pltpu.make_async_copy(source, target.at[0], load_sems.at[j])
        for j, (source, target) in enumerate(own)
    ]
    to_core = [
        remote(source, target.at[1], core_sems, (j,), core)
        for j, (source, target) in enumerate(own)
    ]
    to_across = [
        remote(source, target, y_sems, (j,), across)
        for j, (source, target) in enumerate(
            [(gate_hbm.at[0], w_gate.at[2])]
            + [(up_hbm.at[0, piece(j)], w_up.at[2, piece(j)]) for j in range(UP_PIECES)]
            + [
                (down_hbm.at[0, :, columns(q)], w_down.at[2, :, columns(q)])
                for q in range(CHUNKS)
            ]
            + [(normed_ref.at[portion(j)], other_rows.at[portion(j)]) for j in range(PORTIONS)]
            + [(part_out.at[portion(j)], part_in.at[portion(j)]) for j in range(PORTIONS)]
        )
    ]
    first_down = 1 + UP_PIECES
    rows_across = to_across[first_down + CHUNKS :][:PORTIONS]
    parts_across = to_across[first_down + CHUNKS :][PORTIONS:]
    relayed = [
        remote(source, target, relay_sems, (j,), core)
        for j, (source, target) in enumerate(
            [(w_gate.at[2], w_gate.at[3])]
            + [(w_up.at[2, piece(j)], w_up.at[3, piece(j)]) for j in range(UP_PIECES)]
            + [(w_down.at[2, :, columns(q)], w_down.at[3, :, columns(q)]) for q in range(CHUNKS)]
        )
    ]

    def along(way):
        return {"ep": lax.rem(me + (INNER if way == 0 else n_ep - INNER), n_ep)}

    def block_to(way, index):
        source = blocks.at[way, index - 1] if index else normed_ref
        return remote(source, blocks.at[way, index], block_sems, (way, index), along(way))

    def pieces_to(way, index):
        offset = INNER * index
        owner = lax.rem(me + (n_ep - offset if way == 0 else offset), n_ep)
        return remote(pieces.at[owner], pieces.at[owner], kv_sems, (way, index), along(way))

    def slots_to(j):
        return remote(send.at[j], arrived.at[INNER * j + 1], slot_sems, (j,), beside)

    def pieces_beside(j, owner):
        return remote(pieces.at[owner], pieces.at[owner], kv_side_sems, (j,), beside)

    def table_to(i):
        return remote(tables.at[0], tables.at[i], table_sems, (i,), {"ep": flip(me, i)})

    def side_to(q, j):
        target = plane.at[j, pl.ds(capacity, capacity), columns(q)]
        return remote(sideways.at[j, :, columns(q)], target, side_sems, (q, j), beside)

    def flow_to(q, way, index):
        return remote(
            flow_out.at[way, index, :, columns(q)],
            flow_in.at[way, index, :, columns(q)],
            flow_sems,
            (way, index, q),
            along(way),
        )

    def crossed(a, b):
        result, bit = 0, 1
        while bit < steps:
            differs = lax.rem(lax.rem(lax.div(a, bit), 2) + lax.rem(lax.div(b, bit), 2), 2)
            result, bit = result + bit * differs, 2 * bit
        return result

    def inside(place_at):
        return (place_at >= 0) & (place_at < steps)

    def chosen_by(i, expert):
        base = (expert * capacity).astype(f32)
        index = lax.broadcasted_iota(jnp.int32, (capacity, rows), 0).astype(f32) + base
        return [index == tables[i, k : k + 1, :] for k in range(top)]

    def one_hot(i, expert):
        chosen = chosen_by(i, expert)
        return jnp.where(functools.reduce(jnp.logical_or, chosen), 1.0, 0.0).astype(bf16)

    def spread(block, j):
        packed = jnp.dot(picks[j], block[...], preferred_element_type=f32).astype(bf16)
        arrived[INNER * j] = packed[:capacity]
        send[j] = packed[capacity:]
        slots_to(j).start()

    def pass_on(way, index):
        @pl.when(inside(spot + 1 - 2 * way))
        def _():
            block_to(way, index).start()

    def pieces_on(way, index):
        @pl.when(inside(spot + 1 - 2 * way))
        def _():
            pieces_to(way, index).start()

    def take(distance):
        for way in range(2):
            source = spot - (1 - 2 * way) * distance

            @pl.when(inside(source))
            def _(way=way):
                block_to(way, distance - 1).wait_recv()
                if distance < steps - 1:
                    pass_on(way, distance)

        for way in range(2):
            source = spot - (1 - 2 * way) * distance

            @pl.when(inside(source))
            def _(way=way, source=source):
                spread(blocks.at[way, distance - 1], crossed(spot, source))

        for way in range(2):
            source = spot - (1 - 2 * way) * distance

            @pl.when(inside(source))
            def _(way=way, source=source):
                owner = source * INNER + lax.rem(me, INNER)
                pieces_to(way, distance - 1).wait_recv()
                if distance < steps - 1:
                    pieces_on(way, distance)
                pieces_beside(crossed(spot, source), owner).start()

    barrier = pltpu.get_barrier_semaphore()
    for device in [core, across] + [{"ep": flip(me, i)} for i in range(1, n_ep)]:
        pl.semaphore_signal(barrier, inc=1, device_id=device, device_id_type=MESH)
    for load in small + loads:
        load.start()
    pl.semaphore_wait(barrier, n_ep + 1)
    for copy in to_across[:first_down] + to_core:
        copy.start()

    for load in small:
        load.wait()
    experts = lax.broadcasted_iota(jnp.int32, (n_ep, rows), 0)
    named = [experts == routes_ref[k : k + 1, :] for k in range(top)]
    counted = jnp.where(functools.reduce(jnp.logical_or, named), 1.0, 0.0).astype(bf16)
    at0 = lax.broadcasted_iota(jnp.int32, (rows, rows), 0)
    at1 = lax.broadcasted_iota(jnp.int32, (rows, rows), 1)
    before = jnp.where(at0 < at1, 1.0, 0.0).astype(bf16)
    earlier = jnp.dot(counted, before, preferred_element_type=f32)
    weight_sum = jnp.sum(weights_ref[...], axis=0, keepdims=True)
    for k in range(top):
        rank = jnp.sum(jnp.where(named[k], earlier, 0.0), axis=0, keepdims=True)
        tables[0, k : k + 1, :] = (routes_ref[k : k + 1, :] * capacity).astype(f32) + rank
        tables[0, top + k : top + k + 1, :] = weights_ref[k : k + 1, :] / weight_sum * routed_scale
    for i in range(1, n_ep):
        table_to(i).start()

    for r in range(0, rows, 16):
        values = tokens_ref[r : r + 16, :].astype(f32)
        mean = jnp.mean(values * values, axis=-1, keepdims=True)
        normed_ref[r : r + 16, :] = (values * lax.rsqrt(mean + epsilon) * norm_ref[...]).astype(bf16)
    for way in range(2):
        pass_on(way, 0)

    head = q_gain_ref.shape[1]
    q_heads = q_ref.shape[1] // head
    row_count = q_ref.shape[0]
    position = lax.broadcasted_iota(jnp.int32, (row_count, 2 * head), 0) + me * row_count
    in_lane = lax.broadcasted_iota(jnp.int32, (row_count, 2 * head), 1)
    by_row = lax.rem(in_lane, head) < head // 2
    angle = jnp.where(by_row, lax.div(position, GRID_W), lax.rem(position, GRID_W)).astype(f32)
    angle = angle * freq_ref[...]
    even = lax.rem(in_lane, 2) == 0
    cosine = jnp.cos(angle)
    sine = jnp.where(even, -jnp.sin(angle), jnp.sin(angle))

    def turned(scaled):
        span = scaled.shape[1]
        swapped = jnp.where(even, pltpu.roll(scaled, span - 1, 1), pltpu.roll(scaled, 1, 1))
        return scaled * cosine + swapped * sine

    def factor_of(values):
        return lax.rsqrt(jnp.mean(values * values, axis=-1, keepdims=True) + epsilon)

    key_value = jnp.concatenate([k_ref[...].astype(f32), v_ref[...].astype(f32)], axis=0).T
    key32 = key_value[:, :head]
    key32 = key32 * factor_of(key32) * k_gain_ref[...]
    spun = turned(jnp.concatenate([key32, key_value[:, head:]], axis=1))
    pieces[me] = jnp.where(in_lane < head, spun, key_value).astype(bf16)
    for way in range(2):
        pieces_on(way, 0)
    pieces_beside(0, me).start()

    for i in range(1, n_ep):
        table_to(i).wait()
    for i in range(n_ep):
        chosen = chosen_by(i, me)
        found = 0.0
        for k in range(top):
            found = found + jnp.where(chosen[k], tables[i, top + k : top + k + 1, :], 0.0)
        slot_gates[i * capacity : (i + 1) * capacity, :] = jnp.sum(found, axis=1, keepdims=True)
    for j in range(steps):
        picks[j, :capacity, :] = one_hot(INNER * j, me)
        picks[j, capacity:, :] = one_hot(INNER * j, flip(me, 1))

    spread(normed_ref, 0)
    scale = head ** (-0.5)
    for h in range(0, q_heads, 2):
        pair = [q_ref[:, (h + j) * head : (h + j + 1) * head].astype(f32) for j in range(2)]
        pair = [x * factor_of(x) * q_gain_ref[...] for x in pair]
        spun = turned(jnp.concatenate(pair, axis=1)).astype(bf16) * jnp.asarray(scale, bf16)
        zero = jnp.zeros((row_count, head), bf16)
        for j in range(2):
            q_rot[h + j] = jnp.concatenate([spun[:, j * head : (j + 1) * head], zero], axis=1)

    half = n_ep // 2
    group_rows = half * capacity

    def rows_of(g):
        return arrived[g * half : (g + 1) * half].reshape(group_rows, width)

    def span_of(g):
        return pl.ds(g * group_rows, group_rows)

    def gate_of(p, g):
        gate_acc[p, span_of(g), :] = jnp.dot(rows_of(g), w_gate[p], preferred_element_type=f32)

    def hidden_at(p, g):
        up_proj = jnp.dot(rows_of(g), w_up[p], preferred_element_type=f32)
        gate_proj = gate_acc[p, span_of(g), :]
        hidden[p, span_of(g), :] = (jax.nn.silu(gate_proj) * up_proj).astype(bf16)

    def shared_hidden(source, at, p):
        gate_proj = jnp.dot(source[at, :], s_gate[p], preferred_element_type=f32)
        up_proj = jnp.dot(source[at, :], s_up[p], preferred_element_type=f32)
        s_hidden[p, at, :] = (jax.nn.silu(gate_proj) * up_proj).astype(bf16)

    def shared_down(at, q):
        summed = 0.0
        for p in range(2):
            partial = jnp.dot(
                s_hidden[p, at, :], s_down[p, :, columns(q)], preferred_element_type=f32
            )
            summed = summed + partial.astype(bf16).astype(f32)
        return summed

    def shared_own():
        for p in range(2):
            shared_hidden(normed_ref, pl.ds(0, rows), p)
        for q in range(CHUNKS):
            total[:, columns(q)] = shared_down(pl.ds(0, rows), q)

    def shared_other(j):
        rows_across[j].wait()
        for p in range(2):
            shared_hidden(other_rows, portion(j), p)
        for q in range(CHUNKS):
            part_out[portion(j), columns(q)] = shared_down(portion(j), q).astype(bf16)
        parts_across[j].start()

    for load in loads:
        load.wait()
    for copy in to_core:
        copy.wait()

    block = math.gcd(row_count, 128)

    def attend_head(h):
        def one_block(b, c):
            at = pl.ds(pl.multiple_of(b * block, block), block)
            keys = pieces[...].reshape(n_ep * row_count, 2 * head)
            scores = lax.dot_general(
                q_rot[h, at, :], keys, (((1,), (1,)), ((), ())), preferred_element_type=f32
            )
            weights = jnp.exp(scores - jnp.max(scores, axis=-1, keepdims=True))
            row_sum = jnp.sum(weights, axis=-1, keepdims=True)
            mixed = jnp.dot(weights.astype(bf16), keys, preferred_element_type=f32)
            attn_ref[at, h * head : (h + 1) * head] = (mixed / row_sum)[:, head:].astype(bf16)
            return c

        lax.fori_loop(0, row_count // block, one_block, 0)

    shared_own()
    take(1)
    to_across[0].wait()
    relayed[0].start()
    for copy in to_across[first_down:-PORTIONS]:
        copy.start()
    for j in range(steps // 2):
        slots_to(j).wait()
    for p in range(2):
        gate_of(p, 0)
        hidden_at(p, 0)
    gate_of(2, 0)
    take(2)
    relayed[0].wait()
    gate_of(3, 0)
    for distance in range(3, steps):
        take(distance)
    for j in range(steps // 2, steps):
        slots_to(j).wait()
    for p in range(2):
        gate_of(p, 1)
        hidden_at(p, 1)
    gate_of(2, 1)
    gate_of(3, 1)
    for j in range(1, first_down):
        to_across[j].wait()
        relayed[j].start()
    for g in range(2):
        hidden_at(2, g)
    for j in range(1, first_down):
        relayed[j].wait()
    for g in range(2):
        hidden_at(3, g)

    def forward(q):
        to_across[first_down + q].wait()
        relayed[first_down + q].start()

    def down(q):
        relayed[first_down + q].wait()
        for g in reversed(range(2)):
            summed = 0.0
            for p in range(PARTS):
                partial = jnp.dot(
                    hidden[p, span_of(g), :], w_down[p, :, columns(q)], preferred_element_type=f32
                )
                summed = summed + partial.astype(bf16).astype(f32)
            summed = summed.astype(bf16).astype(f32) * slot_gates[span_of(g), :]
            summed = summed.astype(bf16)
            for j in range(half):
                i = g * half + j
                block = summed[j * capacity : (j + 1) * capacity]
                if i % INNER:
                    sideways[i // INNER, :, columns(q)] = block
                else:
                    plane[i // INNER, :capacity, columns(q)] = block
        for j in reversed(range(steps)):
            side_to(q, j).start()

    def contribution(j, q):
        return lax.dot_general(
            picks[j], plane[j, :, columns(q)], (((0,), (0,)), ((), ())), preferred_element_type=f32
        )

    def emit(q, distance, fed):
        for way in range(2):
            sign = 1 - 2 * way
            target = spot + sign * distance
            behind = inside(spot - sign)

            @pl.when(inside(target) & (behind if fed else jnp.logical_not(behind)))
            def _(way=way, target=target):
                summed = contribution(crossed(spot, target), q)
                if fed:
                    flow_to(q, way, distance).wait_recv()
                    summed = summed + flow_in[way, distance, :, columns(q)].astype(f32)
                flow_out[way, distance - 1, :, columns(q)] = summed.astype(bf16)
                flow_to(q, way, distance - 1).start()

    def edges(q):
        for j in range(steps):
            side_to(q, j).wait()
        for distance in reversed(range(1, steps)):
            emit(q, distance, False)

    def keep(q):
        total[:, columns(q)] += contribution(0, q)
        for way in range(2):

            @pl.when(inside(spot - (1 - 2 * way)))
            def _(way=way):
                flow_to(q, way, 0).wait_recv()
                total[:, columns(q)] += flow_in[way, 0, :, columns(q)].astype(f32)

    def ready(q):
        return 0 <= q < CHUNKS

    forward(0)
    first_head = 2
    for step in range(CHUNKS + steps + 1):
        if ready(step):
            down(step)
        if ready(step - 1):
            edges(step - 1)
        if ready(step + 1):
            forward(step + 1)
        for hop in range(1, steps - 1):
            if ready(step - 1 - hop):
                emit(step - 1 - hop, steps - 1 - hop, True)
        if ready(step - steps):
            keep(step - steps)
        if step == first_head:
            for j in range(steps):
                pieces_beside(j, me).wait()
        if first_head <= step < first_head + q_heads:
            attend_head(step - first_head)
        if 0 <= step - CHUNKS + PORTIONS < PORTIONS:
            shared_other(step - CHUNKS + PORTIONS)

    for copy in parts_across:
        copy.wait()
    for q in range(CHUNKS):
        part = part_in[:, columns(q)].astype(f32)
        moe_ref[:, columns(q)] = (total[:, columns(q)] + part).astype(bf16)
    for way in range(2):
        for index in range(steps - 1):

            @pl.when(inside(spot + 1 - 2 * way) & inside(spot - (1 - 2 * way) * index))
            def _(way=way, index=index):
                pieces_to(way, index).wait_send()
                block_to(way, index).wait_send()

    for way in range(2):
        for distance in range(1, steps):

            @pl.when(inside(spot + (1 - 2 * way) * distance))
            def _(way=way, distance=distance):
                for q in range(CHUNKS):
                    flow_to(q, way, distance - 1).wait_send()


def fused_body(
    query_rows,
    key_rows,
    value_rows,
    query_gain,
    key_gain,
    moe_tokens,
    norm_gain,
    routes,
    route_weights,
    expert_gate,
    expert_up,
    expert_down,
    shared_gate,
    shared_up,
    shared_down,
):
    tok_rows, model_width = moe_tokens.shape
    row_count = query_rows.shape[0]
    head_size = query_gain.shape[0]
    top_count = routes.shape[1]
    ep_size = lax.axis_size("ep")
    capacity = 2 * tok_rows * top_count // ep_size
    units = expert_gate.shape[2]
    steps = ep_size // INNER
    pair_count = head_size // 4
    pair = (np.arange(2 * head_size) % head_size) // 2 % pair_count
    inv_freq = rotary_base ** (-jnp.asarray(pair, jnp.float32) / pair_count)

    bf16, f32 = jnp.bfloat16, jnp.float32
    vmem = pl.BlockSpec(memory_space=pltpu.VMEM)
    dma = pltpu.SemaphoreType.DMA
    all_rows = ep_size * capacity
    token_shape = (tok_rows, model_width)
    small = [
        routes.T,
        route_weights.T,
        moe_tokens,
        norm_gain[None],
        query_rows,
        key_rows.T,
        value_rows.T,
        query_gain[None],
        key_gain[None],
        inv_freq[None],
    ]
    held = [x.shape for x in small]
    held[0] = held[1] = (top_count, tok_rows)
    return pl.pallas_call(
        functools.partial(fused_kernel, (ep_size, capacity, top_count)),
        out_shape=[
            jax.ShapeDtypeStruct(query_rows.shape, bf16),
            jax.ShapeDtypeStruct(moe_tokens.shape, bf16),
        ],
        in_specs=[pl.BlockSpec(memory_space=pltpu.HBM)] * 16,
        out_specs=[vmem] * 2,
        scratch_shapes=[pltpu.VMEM(shape, x.dtype) for shape, x in zip(held, small)]
        + [
            pltpu.VMEM((PARTS, model_width, units), bf16),
            pltpu.VMEM((PARTS, model_width, units), bf16),
            pltpu.VMEM((PARTS, units, model_width), bf16),
            pltpu.VMEM((2, model_width, units), bf16),
            pltpu.VMEM((2, model_width, units), bf16),
            pltpu.VMEM((2, units, model_width), bf16),
            pltpu.VMEM(token_shape, bf16),
            pltpu.VMEM((ep_size, 8, tok_rows), f32),
            pltpu.VMEM((2, steps - 1) + token_shape, bf16),
            pltpu.VMEM((steps, capacity, model_width), bf16),
            pltpu.VMEM((ep_size, capacity, model_width), bf16),
            pltpu.VMEM((all_rows, 1), f32),
            pltpu.VMEM((steps, 2 * capacity, tok_rows), bf16),
            pltpu.VMEM((steps, 2 * capacity, model_width), bf16),
            pltpu.VMEM((steps, capacity, model_width), bf16),
            pltpu.VMEM((2, steps - 1) + token_shape, bf16),
            pltpu.VMEM((2, steps - 1) + token_shape, bf16),
            pltpu.VMEM((PARTS, all_rows, units), bf16),
            pltpu.VMEM((PARTS, all_rows, units), f32),
            pltpu.VMEM((2, tok_rows, units), bf16),
            pltpu.VMEM((ep_size, row_count, 2 * head_size), bf16),
            pltpu.VMEM((query_rows.shape[1] // head_size, row_count, 2 * head_size), bf16),
            pltpu.VMEM(token_shape, bf16),
            pltpu.VMEM(token_shape, bf16),
            pltpu.VMEM(token_shape, bf16),
            pltpu.VMEM(token_shape, f32),
            dma((10,)),
            dma((6,)),
            dma((2, 6)),
            dma((2, 1 + UP_PIECES + CHUNKS + 2 * PORTIONS)),
            dma((2, 1 + UP_PIECES + CHUNKS)),
            dma((2, 2, steps - 1)),
            dma((2, steps)),
            dma((2, ep_size)),
            dma((2, 2, steps - 1)),
            dma((2, steps)),
            dma((2, CHUNKS, steps)),
            dma((2, 2, steps - 1, CHUNKS)),
        ],
        compiler_params=pltpu.CompilerParams(
            collective_id=3, has_side_effects=True, vmem_limit_bytes=VMEM_LIMIT
        ),
    )(
        *small,
        expert_gate,
        expert_up,
        expert_down,
        shared_gate,
        shared_up,
        shared_down,
    )


def body(*arrays):
    query_rows, query_gain, moe_tokens, routes = arrays[0], arrays[3], arrays[5], arrays[7]
    expert_gate = arrays[9]
    ep_size, tp_size = lax.axis_size("ep"), lax.axis_size("tp")
    capacity = 2 * moe_tokens.shape[0] * routes.shape[1] // (ep_size * expert_gate.shape[0])
    head_size = query_gain.shape[0]
    one_kernel = (
        tp_size == PARTS
        and expert_gate.shape[0] == 1
        and ep_size & (ep_size - 1) == 0
        and capacity % 16 == 0
        and ep_size >= 2 * INNER
        and 2 * routes.shape[1] <= 8
        and moe_tokens.shape[0] % 128 == 0
        and ep_size * query_rows.shape[0] * 2 * head_size <= 1 << 20
        and query_rows.shape[1] // head_size % 2 == 0
        and arrays[1].shape[1] == head_size
        and 2 * head_size % 128 == 0
        and math.log2(head_size) % 2 == 0
    )
    return fused_body(*arrays) if one_kernel else plain_body(*arrays)


def solution(mesh):
    return jax.shard_map(
        body,
        mesh=mesh,
        in_specs=(
            P("ep", "tp"),
            P("ep", "tp"),
            P("ep", "tp"),
            P(),
            P(),
            P(("ep", "tp"), None),
            P(),
            P("ep", None),
            P("ep", None),
            P("ep", None, "tp"),
            P("ep", None, "tp"),
            P("ep", "tp", None),
            P(None, "tp"),
            P(None, "tp"),
            P("tp", None),
        ),
        out_specs=(P("ep", "tp"), P(("ep", "tp"), None)),
        check_vma=False,
    )
```
